32 devices in a mesh: tp: 8 (over z, x), dp: 4 (over y, core).
Axes of the slice: x: 2, y: 2, z: 4, core: 2. Of those that a mesh axis runs over, the one named last changes fastest.
Arguments:
- stream: bfloat16 [128, 4096], P(None, 'dp'), may hold values from -12 to 12
- history: int32 [128], P('dp'), may hold values from 1 to 4096, 131072 in all
- input_norm_gain: float32 [2, 4096], P(None, 'dp'), may hold values from 0.1 to 1.9
- query_weight: bfloat16 [2, 4096, 4096], P(None, 'dp', 'tp'), may hold values from -0.09375 to 0.09375
- key_weight: bfloat16 [2, 4096, 4096], P(None, 'dp', 'tp'), may hold values from -0.09375 to 0.09375
- value_weight: bfloat16 [2, 4096, 4096], P(None, 'dp', 'tp'), may hold values from -0.09375 to 0.09375
- gate_weight: bfloat16 [2, 4096, 4096], P(None, 'dp', 'tp'), may hold values from -0.09375 to 0.09375
- adapter_down_weight: bfloat16 [2, 4096, 128], P(None, 'dp'), may hold values from -0.09375 to 0.09375
- decay_up_weight: float32 [2, 64, 4096], P(None, None, 'tp'), may hold values from -3 to 3
- rate_up_weight: float32 [2, 64, 4096], P(None, None, 'tp'), may hold values from -3 to 3
- decay_offset: float32 [2, 4096], P(None, 'tp'), may hold values from -3 to 1
- head_norm_gain: float32 [2, 4096], P(None, 'tp'), may hold values from 0.1 to 1.9
- output_weight: bfloat16 [2, 4096, 4096], P(None, 'tp', 'dp'), may hold values from -0.09375 to 0.09375
- recurrent_state: float32 [2, 128, 64, 4096], P(None, 'dp', 'tp'), may hold values from -5 to 5
Outputs:
- stream_out: bfloat16 [128, 4096], P(None, 'dp')
- state_out: float32 [2, 128, 64, 4096], P(None, 'dp', 'tp')
The draws below stay inside these ranges and needn't reach their ends.
All inputs are finite; a program needn't handle non-finite values. No bound on the sum of `history` on one device may be relied on, other than what follows from the above.
Results may differ from the reference program's by a relative error of at most 0.024.
Values may be sent and summed in bfloat16 or wider, within the bound.
A program may use at most 128 MiB of HBM per device.

```python
import math
import jax
import jax.numpy as jnp
import numpy as np
from jax import lax

MODEL_WIDTH = 4096
HEAD = 64
ADAPTER_RANK = 64
SPAN = 64
BLOCK_COUNT = 2
BATCH = 128
HEADS = 64
N_DP = 4


def draw_stream(key, part):
    first_key, second_key = jax.random.split(jax.random.fold_in(key, 11))
    blocks = 8
    base = jax.random.normal(first_key, (BATCH, MODEL_WIDTH), jnp.float32)
    scales = jnp.exp(jax.random.uniform(second_key, (blocks,), jnp.float32, -1.1, 1.1))
    scales = jnp.repeat(scales, MODEL_WIDTH // blocks)
    return jnp.clip(base * scales[None, :], -12.0, 12.0).astype(jnp.bfloat16)


def level_of(own_key, extent, cuts, low, high):
    def one(position, shards_of):
        draws = jax.random.uniform(jax.random.fold_in(jax.random.fold_in(own_key, 6), position), (shards_of,), jnp.float32, low / len(cuts), high / len(cuts))
        return jnp.repeat(jnp.exp(draws), extent[position] // shards_of).reshape((-1,) + (1,) * (len(extent) - position - 1))

    loudness = one(*cuts[0])
    for cut in cuts[1:]:
        loudness = loudness * one(*cut)
    return loudness


def length_profile(count, total, limit, lean):
    loads = [(1 << 20) // math.isqrt(grade ** lean) + 1 for grade in range(2, count + 1)]
    spare, counts = total - limit - (count - 1), [1] * (count - 1)
    while spare > 0:
        candidates = [i for i in range(count - 1) if counts[i] < limit]
        mass, remaining = sum([loads[i] for i in candidates]), spare
        for i in candidates:
            more = min(limit - counts[i], max(1, remaining * loads[i] // mass), spare)
            counts[i] = counts[i] + more
            spare = spare - more
    return np.array([limit] + counts)


def ragged_sizes(stream_key, count, total, reach, slope):
    if count == 2:
        one = jax.random.randint(stream_key, (), max(1, total - reach), min(reach, total - 1) + 1)
        return jnp.stack([one, total - one])
    lengths = jnp.asarray(length_profile(count, total, reach, slope), jnp.int32)
    pairs = (count - 1) // 2
    donor, taker = lengths[1:1 + 2 * pairs:2], lengths[2:2 + 2 * pairs:2]
    room = jnp.minimum(donor - 1, reach - taker)
    shifted = jax.random.randint(jax.random.fold_in(stream_key, 1), (pairs,), 0, 1 << 20) % (room + 1)
    lengths = lengths.at[1:1 + 2 * pairs:2].set(donor - shifted).at[2:2 + 2 * pairs:2].set(taker + shifted)
    return lengths[jax.random.permutation(jax.random.fold_in(stream_key, 2), count)]


def gaussian(own_key, extent, scale, bound, pieces=(), dtype=jnp.bfloat16):
    entries = scale * jax.random.normal(own_key, extent, jnp.float32)
    if pieces:
        entries = entries * level_of(own_key, extent, pieces, -0.22, 0.18)
    return jnp.clip(entries, -bound, bound).astype(dtype)


def setup_inputs(seed: int = 0) -> dict:
    streams_of = jax.random.split(jax.random.key(seed), 15)
    stream = draw_stream(jax.random.fold_in(streams_of[14], 71), 0)
    history = ragged_sizes(streams_of[1], BATCH, 1024 * BATCH, 4096, 2).astype(jnp.int32)
    input_norm_gain = jnp.clip(1.0 + 0.18 * jax.random.normal(streams_of[2], (BLOCK_COUNT, MODEL_WIDTH), jnp.float32), 0.1, 1.9)
    query_weight = gaussian(streams_of[3], (BLOCK_COUNT, MODEL_WIDTH, MODEL_WIDTH), MODEL_WIDTH ** -0.5, 0.09375, ((1, 4), (2, 8)))
    key_weight = gaussian(streams_of[4], (BLOCK_COUNT, MODEL_WIDTH, MODEL_WIDTH), MODEL_WIDTH ** -0.5, 0.09375, ((1, 4), (2, 8)))
    value_weight = gaussian(streams_of[5], (BLOCK_COUNT, MODEL_WIDTH, MODEL_WIDTH), MODEL_WIDTH ** -0.5, 0.09375, ((1, 4), (2, 8)))
    gate_weight = gaussian(streams_of[6], (BLOCK_COUNT, MODEL_WIDTH, MODEL_WIDTH), MODEL_WIDTH ** -0.5, 0.09375, ((1, 4), (2, 8)))
    adapter_down_weight = gaussian(streams_of[7], (BLOCK_COUNT, MODEL_WIDTH, 2 * ADAPTER_RANK), MODEL_WIDTH ** -0.5, 0.09375, ((1, 4),))
    decay_up_weight = gaussian(streams_of[8], (BLOCK_COUNT, ADAPTER_RANK, MODEL_WIDTH), (ADAPTER_RANK // 16) ** -0.5, 3.0, ((2, 8),), jnp.float32)
    rate_up_weight = gaussian(streams_of[9], (BLOCK_COUNT, ADAPTER_RANK, MODEL_WIDTH), (ADAPTER_RANK // 16) ** -0.5, 3.0, ((2, 8),), jnp.float32)
    decay_offset = jnp.clip(-3.0 + 4.0 * jax.random.uniform(streams_of[10], (BLOCK_COUNT, MODEL_WIDTH), jnp.float32) ** level_of(streams_of[10], (BLOCK_COUNT, MODEL_WIDTH), ((1, 8),), -0.2, 0.2), -3.0, 1.0)
    head_norm_gain = jnp.clip(1.0 + 0.18 * jax.random.normal(streams_of[11], (BLOCK_COUNT, MODEL_WIDTH), jnp.float32), 0.1, 1.9)
    output_weight = gaussian(streams_of[12], (BLOCK_COUNT, MODEL_WIDTH, MODEL_WIDTH), MODEL_WIDTH ** -0.5, 0.09375, ((1, 8), (2, 4)))
    recurrent_state = gaussian(streams_of[13], (BLOCK_COUNT, BATCH, HEADS, HEAD * HEAD), 1.0, 5.0, ((1, 4), (2, 8)), jnp.float32)
    return {"stream": stream, "history": history, "input_norm_gain": input_norm_gain, "query_weight": query_weight, "key_weight": key_weight, "value_weight": value_weight, "gate_weight": gate_weight, "adapter_down_weight": adapter_down_weight, "decay_up_weight": decay_up_weight, "rate_up_weight": rate_up_weight, "decay_offset": decay_offset, "head_norm_gain": head_norm_gain, "output_weight": output_weight, "recurrent_state": recurrent_state}


NORM_EPS = 0.25
GROUP_EPS = 0.25

def projected_rows(rescaled_rows, weight):
    batch_rows = rescaled_rows.shape[0]
    blocked = rescaled_rows.reshape(batch_rows, N_DP, MODEL_WIDTH // N_DP).astype(jnp.float32)
    weight_blocks = weight.reshape(N_DP, MODEL_WIDTH // N_DP, weight.shape[1]).astype(jnp.float32)
    partials = jnp.einsum('bnd,ndc->nbc', blocked, weight_blocks)
    rounded = lax.optimization_barrier(partials.astype(jnp.bfloat16))
    return lax.optimization_barrier(jnp.sum(rounded.astype(jnp.float32), axis=0))

def mixing_block(stream, history, input_norm_gain, query_weight, key_weight, value_weight, gate_weight, adapter_down_weight, decay_up_weight, rate_up_weight, decay_offset, head_norm_gain, output_weight, recurrent_state):
    widened = stream.astype(jnp.float32)
    squares = lax.optimization_barrier(jnp.sum(widened * widened, axis=1))
    inverse_root_mean = lax.rsqrt(squares / MODEL_WIDTH + NORM_EPS)[:, None]
    rescaled_rows = (widened * input_norm_gain[None, :]).astype(jnp.bfloat16)
    query = projected_rows(rescaled_rows, query_weight) * inverse_root_mean
    key_proj = projected_rows(rescaled_rows, key_weight) * inverse_root_mean
    value_proj = projected_rows(rescaled_rows, value_weight) * inverse_root_mean
    gate_pre = projected_rows(rescaled_rows, gate_weight) * inverse_root_mean
    adapter_hidden = projected_rows(rescaled_rows, adapter_down_weight) * inverse_root_mean
    pos_factor = 0.5 + (history // SPAN % 3).astype(jnp.float32)
    decay_logits = decay_offset[None, :] + jnp.dot(jnp.tanh(adapter_hidden[:, :ADAPTER_RANK]), decay_up_weight, precision=lax.Precision.HIGHEST)
    rate_log = -jax.nn.softplus(-decay_logits) - 0.5
    decay = jnp.exp(-jnp.exp(rate_log) * pos_factor[:, None])
    learning_rate = jax.nn.sigmoid(jnp.dot(adapter_hidden[:, ADAPTER_RANK:], rate_up_weight, precision=lax.Precision.HIGHEST))
    batch_rows = widened.shape[0]
    head_count = MODEL_WIDTH // HEAD

    def heads_of(values):
        return values.reshape(batch_rows, head_count, HEAD)
    keys = heads_of(key_proj)
    key_unit = keys * lax.rsqrt(lax.optimization_barrier(jnp.sum(keys * keys, axis=-1, keepdims=True)) + 1.0)
    key_rate = key_unit * heads_of(learning_rate)
    matrix = recurrent_state.reshape(batch_rows, head_count, HEAD, HEAD)
    state_key = jnp.einsum('bhvk,bhk->bhv', matrix, key_unit)
    refreshed_state = matrix * heads_of(decay)[:, :, None, :] - state_key[..., None] * key_rate[:, :, None, :] + heads_of(value_proj)[..., None] * keys[:, :, None, :]
    readout = jnp.einsum('bhvk,bhk->bhv', refreshed_state, heads_of(query))
    mean_y = lax.optimization_barrier(jnp.mean(readout, axis=-1, keepdims=True))
    spread = lax.optimization_barrier(jnp.mean(jnp.square(readout - mean_y), axis=-1, keepdims=True))
    normed = ((readout - mean_y) * lax.rsqrt(spread + GROUP_EPS)).reshape(batch_rows, MODEL_WIDTH) * head_norm_gain[None, :]
    mixed = (normed * jax.nn.sigmoid(gate_pre)).astype(jnp.bfloat16)
    out_sum = jnp.dot(mixed, output_weight, preferred_element_type=jnp.float32)
    return ((widened + out_sum).astype(jnp.bfloat16), refreshed_state.reshape(batch_rows, head_count, HEAD * HEAD))

def reference(stream, history, input_norm_gain, query_weight, key_weight, value_weight, gate_weight, adapter_down_weight, decay_up_weight, rate_up_weight, decay_offset, head_norm_gain, output_weight, recurrent_state):
    new_states = []
    for layer_lookup in range(BLOCK_COUNT):
        stream, refreshed_state = mixing_block(stream, history, input_norm_gain[layer_lookup], query_weight[layer_lookup], key_weight[layer_lookup], value_weight[layer_lookup], gate_weight[layer_lookup], adapter_down_weight[layer_lookup], decay_up_weight[layer_lookup], rate_up_weight[layer_lookup], decay_offset[layer_lookup], head_norm_gain[layer_lookup], output_weight[layer_lookup], recurrent_state[layer_lookup])
        new_states.append(refreshed_state)
    return (stream, jnp.stack(new_states))
```

```python
import functools

import jax
import jax.numpy as jnp
from jax import lax
from jax.experimental import pallas as pl
from jax.experimental.pallas import tpu as pltpu
from jax.sharding import PartitionSpec as P

HEAD = 64
SPAN = 64
BLOCK_COUNT = 2
LANES = 128
NORM_EPS = 0.25
GROUP_EPS = 0.25
DECAY_SCALE = 0.6065306597126334
TILE = 256
FLUSHES = 8
MESH = pl.DeviceIdType.MESH
F32 = jnp.float32
BF16 = jnp.bfloat16


def sigmoid(z):
    e = jnp.exp(-jnp.abs(z))
    return jnp.where(z >= 0, 1.0, e) / (1.0 + e)


def kernel(
    n_dp,
    n_tp,
    halves,
    stream_ref,
    history_ref,
    in_gain,
    adapter_hbm,
    key_hbm,
    query_hbm,
    value_hbm,
    gate_hbm,
    decay_up,
    rate_up,
    offset,
    head_gain,
    out_hbm,
    state_hbm,
    stream_out,
    state,
    wa,
    wk,
    wq,
    wv,
    wg,
    wo,
    sent,
    got,
    sq_sent,
    sq_got,
    mixed_all,
    terms,
    terms_got,
    fresh,
    x_ref,
    rows,
    splits,
    gather1,
    gather2,
    spread,
    load_sem,
    rs_send,
    rs_recv,
    sq_send,
    sq_recv,
    ag_send,
    ag_recv,
    tr_send,
    tr_recv,
    ta_send,
    ta_recv,
):
    me = lax.axis_index("dp")
    lane_me = lax.axis_index("tp")
    batch, depth = stream_ref.shape
    seq = batch // n_dp
    width = wk.shape[2]
    heads = width // HEAD
    span = batch // halves
    own = seq // halves
    count = own * heads
    part = span // n_tp
    rank = wa.shape[2] // 2
    vk = state.shape[2]
    tiles = vk // TILE
    lanes = sq_sent.shape[3]

    loads = {}

    def load(l, i, src, dst):
        loads[l, i] = pltpu.make_async_copy(src.at[l], dst.at[l], load_sem.at[l, i])
        loads[l, i].start()

    def load_in(l):
        load(l, 0, adapter_hbm, wa)
        load(l, 1, key_hbm, wk)
        load(l, 2, query_hbm, wq)
        load(l, 3, value_hbm, wv)
        load(l, 4, gate_hbm, wg)

    def load_rest(l):
        load(l, 5, state_hbm, state)
        load(l, 6, out_hbm, wo)

    load_in(0)
    load_rest(0)

    def dp_peer(o):
        return lax.rem(me + o, n_dp)

    def tp_peer(o):
        return lax.rem(lane_me + o, n_tp)

    barrier = pltpu.get_barrier_semaphore()
    for o in range(1, n_dp):
        pl.semaphore_signal(barrier, inc=1, device_id={"dp": dp_peer(o)}, device_id_type=MESH)
    for o in range(1, n_tp):
        pl.semaphore_signal(barrier, inc=1, device_id={"tp": tp_peer(o)}, device_id_type=MESH)

    def fill(t, carry):
        at = pl.ds(pl.multiple_of(t * TILE, TILE), TILE)
        r = (lax.broadcasted_iota(jnp.int32, (TILE, LANES), 0) + t * TILE) // HEAD
        c = lax.broadcasted_iota(jnp.int32, (TILE, LANES), 1)
        gather1[at, :] = jnp.where(r == c, 1.0, 0.0).astype(BF16)
        gather2[at, :] = jnp.where(r + HEAD == c, 1.0, 0.0).astype(BF16)
        r = lax.broadcasted_iota(jnp.int32, (LANES, TILE), 0)
        c = (lax.broadcasted_iota(jnp.int32, (LANES, TILE), 1) + t * TILE) // HEAD
        spread[:, at] = jnp.where((r == c) | (r == c + HEAD), 1.0, 0.0).astype(BF16)
        return carry

    low = lax.broadcasted_iota(jnp.int32, (own, LANES), 1) < HEAD
    low_rows = lax.broadcasted_iota(jnp.int32, (count, LANES), 1) < HEAD

    def to_rows(value, h, i):
        buf = rows.at[h, i]
        for j in range(width // LANES):
            pair = value[:, j * LANES : (j + 1) * LANES]
            turned = pltpu.roll(pair, HEAD, 1)
            buf[pl.ds(2 * j, own, stride=heads), :] = jnp.where(low, pair, turned)
            buf[pl.ds(2 * j + 1, own, stride=heads), :] = jnp.where(low, turned, pair)
        return rows[h, i]

    def half_sum(v):
        return jnp.sum(v, axis=1, keepdims=True) * 0.5

    def twice(v):
        return jnp.concatenate([v, v], axis=1)

    for h in range(halves):
        for d in range(n_dp):
            x_ref[h, d * own : (d + 1) * own, :] = stream_ref[d * seq + h * own : d * seq + (h + 1) * own, :].astype(F32)
    spans = jnp.floor(history_ref[...].astype(F32) * (1.0 / SPAN))
    phase = 0.5 + (spans - 3.0 * jnp.floor((spans + 0.5) * (1.0 / 3.0)))
    diagonal = lax.broadcasted_iota(jnp.int32, (seq, seq), 0) == lax.broadcasted_iota(jnp.int32, (seq, seq), 1)
    pos = jnp.sum(jnp.where(diagonal, phase, 0.0), axis=1, keepdims=True)
    mine = pl.ds(pl.multiple_of(me * own, own), own)
    own_part = pl.ds(pl.multiple_of(lane_me * part, part), part)
    row_at = lax.broadcasted_iota(jnp.int32, (span, lanes), 0)
    diag = row_at == lax.broadcasted_iota(jnp.int32, (span, lanes), 1)
    own_at = lax.broadcasted_iota(jnp.int32, (own, lanes), 0) + me * own
    own_diag = own_at == lax.broadcasted_iota(jnp.int32, (own, lanes), 1)
    sizes = [2 * rank, width, width, width, width]
    starts = [sum(sizes[:c]) for c in range(5)]
    pending = []

    def remote(src, dst, send, recv, where):
        copy = pltpu.make_async_remote_copy(
            src_ref=src, dst_ref=dst, send_sem=send, recv_sem=recv, device_id=where, device_id_type=MESH
        )
        copy.start()
        pending.append(copy)
        return copy

    copies = {}

    def project(l, h):
        x = x_ref[h]
        column = jnp.sum(x * x, axis=1, keepdims=True)
        line = jnp.sum(jnp.where(diag, column, 0.0), axis=0, keepdims=True)
        sq_sent[l, h] = jnp.broadcast_to(line, (8, lanes))
        scaled = (x * in_gain[l : l + 1, :]).astype(BF16)
        if l == 0 and h == 0:
            pl.semaphore_wait(barrier, n_dp + n_tp - 2)
        for o in range(1, n_dp):
            copies["sq", l, h, o] = remote(
                sq_sent.at[l, h],
                sq_got.at[l, h, o - 1],
                sq_send.at[l, h, o - 1],
                sq_recv.at[l, h, o - 1],
                {"dp": dp_peer(o)},
            )
        for c, weight in enumerate((wa, wk, wq, wv, wg)):
            if h == 0:
                loads[l, c].wait()
            cols = pl.ds(starts[c], sizes[c])
            sent[l, h, :, cols] = jnp.dot(scaled, weight[l], preferred_element_type=F32).astype(BF16)
            for o in range(1, n_dp):
                there = dp_peer(o)
                at = pl.ds(pl.multiple_of(there * own, own), own)
                copies["rs", l, h, c, o] = remote(
                    sent.at[l, h, at, cols],
                    got.at[l, h, o - 1, :, cols],
                    rs_send.at[l, h, c, o - 1],
                    rs_recv.at[l, h, c, o - 1],
                    {"dp": there},
                )

    def mix(l, h):
        for o in range(1, n_dp):
            copies["sq", l, h, o].wait_recv()
        line = sq_sent[l, h]
        for o in range(1, n_dp):
            line = line + sq_got[l, h, o - 1]
        squares = jnp.sum(jnp.where(own_diag, line[:1, :], 0.0), axis=1, keepdims=True)
        inv_rms = lax.rsqrt(squares / (depth * n_dp) + NORM_EPS)

        def total(c):
            for o in range(1, n_dp):
                copies["rs", l, h, c, o].wait_recv()
            cols = pl.ds(starts[c], sizes[c])
            out = sent[l, h, mine, cols].astype(F32)
            for o in range(1, n_dp):
                out = out + got[l, h, o - 1, :, cols].astype(F32)
            return out * inv_rms

        low_rank = total(0)
        z = offset[l : l + 1, :] + jnp.dot(
            jnp.tanh(low_rank[:, :rank]), decay_up[l], precision=lax.Precision.HIGHEST, preferred_element_type=F32
        )
        decay = to_rows(jnp.exp(sigmoid(z) * (-DECAY_SCALE) * pos[h * own : (h + 1) * own, :]), h, 0)
        learn = to_rows(
            sigmoid(
                jnp.dot(low_rank[:, rank:], rate_up[l], precision=lax.Precision.HIGHEST, preferred_element_type=F32)
            ),
            h,
            1,
        )
        keys = to_rows(total(1), h, 2)
        key_unit = keys * lax.rsqrt(half_sum(keys * keys) + 1.0)
        key_rate = key_unit * learn
        rows[h, 1] = key_rate
        query = to_rows(total(2), h, 3)
        key_query = half_sum(keys * query)
        rate_query = half_sum(key_rate * query)
        unit2 = twice(key_unit)
        query2 = twice(decay * query)
        if h == 0:
            loads[l, 5].wait()

        def products(t, acc):
            at = pl.ds(pl.multiple_of(t * TILE, TILE), TILE)
            s = state[l, h * count : (h + 1) * count, at]
            return (
                acc
                + jnp.dot((s * unit2).astype(BF16), gather1[at, :], preferred_element_type=F32)
                + jnp.dot((s * query2).astype(BF16), gather2[at, :], preferred_element_type=F32)
            )

        acc = lax.fori_loop(0, tiles, products, jnp.zeros((count, LANES), F32), unroll=True)
        turned = pltpu.roll(acc, HEAD, 1)
        state_key = jnp.where(low_rows, acc, turned)
        from_state = jnp.where(low_rows, turned, acc)
        value = to_rows(total(3), h, 4)
        readout = from_state - state_key * rate_query + value * key_query
        mean = half_sum(readout) * (1.0 / HEAD)
        centred = readout - mean
        var = half_sum(centred * centred) * (1.0 / HEAD)
        rows[h, 5] = centred * lax.rsqrt(var + GROUP_EPS)
        gate = sigmoid(total(4)) * head_gain[l : l + 1, :]
        normed = rows.at[h, 5]
        for j in range(width // LANES):
            even = normed[pl.ds(2 * j, own, stride=heads), :]
            odd = normed[pl.ds(2 * j + 1, own, stride=heads), :]
            cols = slice(j * LANES, (j + 1) * LANES)
            mixed_all[l, h, mine, cols] = (jnp.where(low, even, odd) * gate[:, cols]).astype(BF16)
        for o in range(1, n_dp):
            copies["ag", l, h, o] = remote(
                mixed_all.at[l, h, mine],
                mixed_all.at[l, h, mine],
                ag_send.at[l, h, o - 1],
                ag_recv.at[l, h, o - 1],
                {"dp": dp_peer(o)},
            )

        def split(v):
            high = v.astype(BF16)
            rest = (v - high.astype(F32)).astype(BF16)
            return jnp.where(low_rows, high.astype(F32), rest.astype(F32)).astype(BF16)

        splits[h, 0] = split(value)
        splits[h, 1] = split(state_key)

    def update(l, h, first, last):
        def one(t, carry):
            at = pl.ds(pl.multiple_of(t * TILE, TILE), TILE)
            wide = jnp.dot(splits[h, 0], spread[:, at], preferred_element_type=F32)
            drop = jnp.dot(splits[h, 1], spread[:, at], preferred_element_type=F32)
            block = slice(h * count, (h + 1) * count)
            state[l, block, at] = (
                state[l, block, at] * twice(rows[h, 0]) - drop * twice(rows[h, 1]) + wide * twice(rows[h, 2])
            )
            return carry

        lax.fori_loop(first, last, one, 0, unroll=True)

    def output(l, h):
        for o in range(1, n_dp):
            copies["ag", l, h, o].wait_recv()
        if h == 0:
            loads[l, 6].wait()
        product = jnp.dot(mixed_all[l, h], wo[l], preferred_element_type=F32)
        terms[l, h] = product.reshape(n_tp, part, depth).astype(BF16)
        for o in range(1, n_tp):
            there = tp_peer(o)
            copies["tr", l, h, o] = remote(
                terms.at[l, h, there],
                terms_got.at[l, h, o - 1],
                tr_send.at[l, h, o - 1],
                tr_recv.at[l, h, o - 1],
                {"tp": there},
            )

    def gather_terms(l, h):
        acc = terms[l, h, lane_me].astype(F32)
        for o in range(1, n_tp):
            copies["tr", l, h, o].wait_recv()
            acc = acc + terms_got[l, h, o - 1].astype(F32)
        fresh[l, h, lane_me] = (x_ref[h, own_part, :] + acc).astype(BF16)
        for o in range(1, n_tp):
            copies["ta", l, h, o] = remote(
                fresh.at[l, h, lane_me],
                fresh.at[l, h, lane_me],
                ta_send.at[l, h, o - 1],
                ta_recv.at[l, h, o - 1],
                {"tp": tp_peer(o)},
            )

    def renew(l, h):
        for o in range(1, n_tp):
            copies["ta", l, h, o].wait_recv()
        if l + 1 < BLOCK_COUNT:
            x_ref[h] = fresh[l, h].astype(F32).reshape(span, depth)
        else:
            last = fresh[l, h].reshape(span, depth)
            for d in range(n_dp):
                stream_out[d * seq + h * own : d * seq + (h + 1) * own, :] = last[d * own : (d + 1) * own, :]

    every = range(halves)
    cut = [tiles * i // 4 for i in range(5)]
    for l in range(BLOCK_COUNT):
        for h in every:
            if l > 0:
                renew(l - 1, h)
            project(l, h)
        if l == 0:
            lax.fori_loop(0, tiles, fill, 0)
        if l + 1 < BLOCK_COUNT:
            load_in(l + 1)
            load_rest(l + 1)
        for h in every:
            mix(l, h)
        for h in every:
            update(l, h, cut[0], cut[1])
            output(l, h)
        for h in every:
            update(l, h, cut[1], cut[2])
        for h in every:
            update(l, h, cut[2], cut[3])
            gather_terms(l, h)
        for h in every:
            update(l, h, cut[3], cut[4])
    for h in every:
        renew(BLOCK_COUNT - 1, h)
    for copy in pending:
        copy.wait_send()


def flush(out, state, out_hbm, state_hbm, sem):
    copies = [pltpu.make_async_copy(out, out_hbm, sem.at[0])]
    for i in range(FLUSHES):
        rows = state.shape[1] // FLUSHES
        at = pl.ds(i * rows, rows)
        copies.append(pltpu.make_async_copy(state.at[:, at], state_hbm.at[:, at], sem.at[i + 1]))
    for copy in copies:
        copy.start()
    for copy in copies:
        copy.wait()


def solution(mesh):
    n_dp, n_tp = mesh.shape["dp"], mesh.shape["tp"]

    def body(
        stream,
        history,
        input_norm_gain,
        query_weight,
        key_weight,
        value_weight,
        gate_weight,
        adapter_down_weight,
        decay_up_weight,
        rate_up_weight,
        decay_offset,
        head_norm_gain,
        output_weight,
        recurrent_state,
    ):
        batch, depth = stream.shape
        width = query_weight.shape[2]
        blocks, seq, heads, vk = recurrent_state.shape
        count = seq * heads
        halves = 2 if batch % (2 * 8 * n_tp) == 0 and seq % 32 == 0 else 1
        span = batch // halves
        own = seq // halves
        part = span // n_tp
        lanes = (span + LANES - 1) // LANES * LANES
        columns = 4 * width + adapter_down_weight.shape[2]
        vmem = pl.BlockSpec(memory_space=pltpu.VMEM)
        hbm = pl.BlockSpec(memory_space=pl.ANY)
        dma = pltpu.SemaphoreType.DMA

        def like(w):
            return pltpu.VMEM(w.shape, w.dtype)

        out, new_state = pl.pallas_call(
            functools.partial(kernel, n_dp, n_tp, halves),
            out_shape=(
                pltpu.VMEM((batch, depth), BF16),
                pltpu.VMEM((blocks, count, vk), F32),
            ),
            in_specs=[vmem] * 3 + [hbm] * 5 + [vmem] * 4 + [hbm] * 2,
            out_specs=(vmem, vmem),
            scratch_shapes=[
                like(adapter_down_weight),
                like(key_weight),
                like(query_weight),
                like(value_weight),
                like(gate_weight),
                like(output_weight),
                pltpu.VMEM((blocks, halves, span, columns), BF16),
                pltpu.VMEM((blocks, halves, n_dp - 1, own, columns), BF16),
                pltpu.VMEM((blocks, halves, 8, lanes), F32),
                pltpu.VMEM((blocks, halves, n_dp - 1, 8, lanes), F32),
                pltpu.VMEM((blocks, halves, span, width), BF16),
                pltpu.VMEM((blocks, halves, n_tp, part, depth), BF16),
                pltpu.VMEM((blocks, halves, n_tp - 1, part, depth), BF16),
                pltpu.VMEM((blocks, halves, n_tp, part, depth), BF16),
                pltpu.VMEM((halves, span, depth), F32),
                pltpu.VMEM((halves, 6, count // halves, LANES), F32),
                pltpu.VMEM((halves, 2, count // halves, LANES), BF16),
                pltpu.VMEM((vk, LANES), BF16),
                pltpu.VMEM((vk, LANES), BF16),
                pltpu.VMEM((LANES, vk), BF16),
                dma((blocks, 7)),
                dma((blocks, halves, 5, n_dp - 1)),
                dma((blocks, halves, 5, n_dp - 1)),
                dma((blocks, halves, n_dp - 1)),
                dma((blocks, halves, n_dp - 1)),
                dma((blocks, halves, n_dp - 1)),
                dma((blocks, halves, n_dp - 1)),
                dma((blocks, halves, n_tp - 1)),
                dma((blocks, halves, n_tp - 1)),
                dma((blocks, halves, n_tp - 1)),
                dma((blocks, halves, n_tp - 1)),
            ],
            compiler_params=pltpu.CompilerParams(
                collective_id=0, has_side_effects=True, vmem_limit_bytes=54 * 1024 * 1024
            ),
        )(
            stream,
            history[None, :],
            input_norm_gain,
            adapter_down_weight,
            key_weight,
            query_weight,
            value_weight,
            gate_weight,
            decay_up_weight,
            rate_up_weight,
            decay_offset,
            head_norm_gain,
            output_weight,
            recurrent_state.reshape(blocks, count, vk),
        )
        out, new_state = pl.pallas_call(
            flush,
            out_shape=(
                jax.ShapeDtypeStruct((batch, depth), BF16),
                jax.ShapeDtypeStruct((blocks, count, vk), F32),
            ),
            in_specs=[hbm, hbm],
            out_specs=(hbm, hbm),
            scratch_shapes=[dma((FLUSHES + 1,))],
            compiler_params=pltpu.CompilerParams(vmem_limit_bytes=1024 * 1024),
        )(out, new_state)
        return out, new_state.reshape(blocks, seq, heads, vk)

    placed = (
        P(None, "dp"),
        P("dp"),
        P(None, "dp"),
        P(None, "dp", "tp"),
        P(None, "dp", "tp"),
        P(None, "dp", "tp"),
        P(None, "dp", "tp"),
        P(None, "dp", None),
        P(None, None, "tp"),
        P(None, None, "tp"),
        P(None, "tp"),
        P(None, "tp"),
        P(None, "tp", "dp"),
        P(None, "dp", "tp", None),
    )
    return jax.shard_map(
        body,
        mesh=mesh,
        in_specs=placed,
        out_specs=(P(None, "dp"), P(None, "dp", "tp", None)),
        check_vma=False,
    )
```

```python
import functools

import jax
import jax.numpy as jnp
from jax import lax
from jax.experimental import pallas as pl
from jax.experimental.pallas import tpu as pltpu
from jax.sharding import PartitionSpec as P

HEAD = 64
SPAN = 64
BLOCK_COUNT = 2
LANES = 128
NORM_EPS = 0.25
GROUP_EPS = 0.25
DECAY_SCALE = 0.6065306597126334
TILE = 256
FLUSHES = 8
PIECES = 2
MESH = pl.DeviceIdType.MESH
F32 = jnp.float32
BF16 = jnp.bfloat16


def sigmoid(z):
    e = jnp.exp(-jnp.abs(z))
    return jnp.where(z >= 0, 1.0, e) / (1.0 + e)


def kernel(
    n_dp,
    n_tp,
    halves,
    stream_hbm,
    history_hbm,
    in_gain_hbm,
    adapter_hbm,
    key_hbm,
    query_hbm,
    value_hbm,
    gate_hbm,
    decay_up_hbm,
    rate_up_hbm,
    offset_hbm,
    head_gain_hbm,
    out_hbm,
    state_hbm,
    stream_out,
    state,
    stream_ref,
    history_ref,
    in_gain,
    decay_up,
    rate_up,
    offset,
    head_gain,
    wa,
    wk,
    wq,
    wv,
    wg,
    wo,
    sent,
    got,
    sq_sent,
    sq_got,
    mixed_all,
    terms,
    terms_got,
    fresh,
    x_ref,
    rows,
    splits,
    gather1,
    gather2,
    spread,
    small_sem,
    load_sem,
    rs_send,
    rs_recv,
    sq_send,
    sq_recv,
    ag_send,
    ag_recv,
    tr_send,
    tr_recv,
    ta_send,
    ta_recv,
):
    me = lax.axis_index("dp")
    lane_me = lax.axis_index("tp")
    batch, depth = stream_ref.shape
    seq = batch // n_dp
    width = wk.shape[2]
    heads = width // HEAD
    span = batch // halves
    own = seq // halves
    count = own * heads
    rank = wa.shape[2] // 2
    vk = state.shape[2]
    tiles = vk // TILE
    lanes = sq_sent.shape[3]
    reducers, part_rows, part_cols = terms.shape[2:]
    first = (n_tp - reducers) // 2
    strips = depth // part_cols

    def dp_peer(o):
        return lax.rem(me + o, n_dp)

    def tp_peer(o):
        return lax.rem(lane_me + o, n_tp)

    barrier = pltpu.get_barrier_semaphore()
    for o in range(1, n_tp):
        pl.semaphore_signal(barrier, inc=1, device_id={"tp": tp_peer(o)}, device_id_type=MESH)
    for o in range(1, n_dp):
        pl.semaphore_signal(barrier, inc=1, device_id={"dp": dp_peer(o)}, device_id_type=MESH)

    loads = {}
    small = []

    def load(l, i, src, dst):
        loads[l, i] = pltpu.make_async_copy(src.at[l], dst.at[l], load_sem.at[l, i])
        loads[l, i].start()

    def load_small(src, dst):
        small.append(pltpu.make_async_copy(src, dst, small_sem.at[len(small)]))
        small[-1].start()

    def load_in(l):
        load(l, 0, adapter_hbm, wa)
        load(l, 1, key_hbm, wk)
        load(l, 2, query_hbm, wq)
        load(l, 3, value_hbm, wv)
        load(l, 4, gate_hbm, wg)

    def load_rest(l):
        load(l, 5, state_hbm, state)
        load(l, 6, out_hbm, wo)

    load_small(stream_hbm, stream_ref)
    load_small(in_gain_hbm, in_gain)
    load_in(0)
    load_small(history_hbm, history_ref)
    load_small(decay_up_hbm, decay_up)
    load_small(rate_up_hbm, rate_up)
    load_small(offset_hbm, offset)
    load_small(head_gain_hbm, head_gain)
    load_rest(0)

    def fill(t, carry):
        at = pl.ds(pl.multiple_of(t * TILE, TILE), TILE)
        r = (lax.broadcasted_iota(jnp.int32, (TILE, LANES), 0) + t * TILE) // HEAD
        c = lax.broadcasted_iota(jnp.int32, (TILE, LANES), 1)
        gather1[at, :] = jnp.where(r == c, 1.0, 0.0).astype(BF16)
        gather2[at, :] = jnp.where(r + HEAD == c, 1.0, 0.0).astype(BF16)
        r = lax.broadcasted_iota(jnp.int32, (LANES, TILE), 0)
        c = (lax.broadcasted_iota(jnp.int32, (LANES, TILE), 1) + t * TILE) // HEAD
        spread[:, at] = jnp.where((r == c) | (r == c + HEAD), 1.0, 0.0).astype(BF16)
        return carry

    low = lax.broadcasted_iota(jnp.int32, (own, LANES), 1) < HEAD
    low_rows = lax.broadcasted_iota(jnp.int32, (count, LANES), 1) < HEAD

    def to_rows(value, h, i):
        buf = rows.at[h, i]
        for j in range(width // LANES):
            pair = value[:, j * LANES : (j + 1) * LANES]
            turned = pltpu.roll(pair, HEAD, 1)
            buf[pl.ds(2 * j, own, stride=heads), :] = jnp.where(low, pair, turned)
            buf[pl.ds(2 * j + 1, own, stride=heads), :] = jnp.where(low, turned, pair)
        return rows[h, i]

    def half_sum(v):
        return jnp.sum(v, axis=1, keepdims=True) * 0.5

    def twice(v):
        return jnp.concatenate([v, v], axis=1)

    mine = pl.ds(pl.multiple_of(me * own, own), own)
    row_at = lax.broadcasted_iota(jnp.int32, (span, lanes), 0)
    diag = row_at == lax.broadcasted_iota(jnp.int32, (span, lanes), 1)
    own_at = lax.broadcasted_iota(jnp.int32, (own, lanes), 0) + me * own
    own_diag = own_at == lax.broadcasted_iota(jnp.int32, (own, lanes), 1)
    sizes = [2 * rank, width, width, width, width]
    starts = [sum(sizes[:c]) for c in range(5)]
    copies = {}

    def describe(key, src, dst, send, recv, where):
        copies[key] = pltpu.make_async_remote_copy(
            src_ref=src, dst_ref=dst, send_sem=send, recv_sem=recv, device_id=where, device_id_type=MESH
        )
        return copies[key]

    def send_squares(l, h):
        for o in range(1, n_dp):
            describe(
                ("sq", l, h, o),
                sq_sent.at[l, h],
                sq_got.at[l, h, o - 1],
                sq_send.at[l, h, o - 1],
                sq_recv.at[l, h, o - 1],
                {"dp": dp_peer(o)},
            ).start()

    def send_columns(l, h, c):
        cols = pl.ds(starts[c], sizes[c])
        for o in range(1, n_dp):
            there = dp_peer(o)
            at = pl.ds(pl.multiple_of(there * own, own), own)
            describe(
                ("rs", l, h, c, o),
                sent.at[l, h, at, cols],
                got.at[l, h, o - 1, :, cols],
                rs_send.at[l, h, c, o - 1],
                rs_recv.at[l, h, c, o - 1],
                {"dp": there},
            ).start()

    def put_squares(l, h, x):
        column = jnp.sum(x * x, axis=1, keepdims=True)
        line = jnp.sum(jnp.where(diag, column, 0.0), axis=0, keepdims=True)
        sq_sent[l, h] = jnp.broadcast_to(line, (8, lanes))

    weights = (wa, wk, wq, wv, wg)

    def project_all():
        small[0].wait()
        small[1].wait()
        for h in range(halves):
            for d in range(n_dp):
                x_ref[h, d * own : (d + 1) * own, :] = stream_ref[
                    d * seq + h * own : d * seq + (h + 1) * own, :
                ]
        for h in range(halves):
            put_squares(0, h, x_ref[h].astype(F32))
        x = x_ref[...].reshape(batch, depth).astype(F32)
        scaled = (x * in_gain[:1, :]).astype(BF16)
        for c, weight in enumerate(weights):
            loads[0, c].wait()
            cols = pl.ds(starts[c], sizes[c])
            product = jnp.dot(scaled, weight[0], preferred_element_type=F32).astype(BF16)
            sent[0, :, :, cols] = product.reshape(halves, span, sizes[c])
        pl.semaphore_wait(barrier, n_dp + n_tp - 2)
        for h in range(halves):
            send_squares(0, h)
            for c in range(len(weights)):
                send_columns(0, h, c)

    def project(l, h):
        rows_of = []
        for i in range(reducers // strips):
            strip = [fresh[l - 1, h, i * strips + j] for j in range(strips)]
            rows_of.append(jnp.concatenate(strip, axis=1))
        x = jnp.concatenate(rows_of, axis=0).astype(F32)
        put_squares(l, h, x)
        scaled = (x * in_gain[l : l + 1, :]).astype(BF16)
        send_squares(l, h)
        for c, weight in enumerate(weights):
            if h == 0:
                loads[l, c].wait()
            cols = pl.ds(starts[c], sizes[c])
            sent[l, h, :, cols] = jnp.dot(scaled, weight[l], preferred_element_type=F32).astype(BF16)
            send_columns(l, h, c)

    def prepare():
        for copy in small[2:]:
            copy.wait()
        spans = jnp.floor(history_ref[...].astype(F32) * (1.0 / SPAN))
        phase = 0.5 + (spans - 3.0 * jnp.floor((spans + 0.5) * (1.0 / 3.0)))
        diagonal = lax.broadcasted_iota(jnp.int32, (seq, seq), 0) == lax.broadcasted_iota(jnp.int32, (seq, seq), 1)
        return jnp.sum(jnp.where(diagonal, phase, 0.0), axis=1, keepdims=True)

    def mix(l, h):
        for o in range(1, n_dp):
            copies["sq", l, h, o].wait_recv()
        line = sq_sent[l, h]
        for o in range(1, n_dp):
            line = line + sq_got[l, h, o - 1]
        squares = jnp.sum(jnp.where(own_diag, line[:1, :], 0.0), axis=1, keepdims=True)
        inv_rms = lax.rsqrt(squares / (depth * n_dp) + NORM_EPS)

        def total(c):
            for o in range(1, n_dp):
                copies["rs", l, h, c, o].wait_recv()
            cols = pl.ds(starts[c], sizes[c])
            out = sent[l, h, mine, cols].astype(F32)
            for o in range(1, n_dp):
                out = out + got[l, h, o - 1, :, cols].astype(F32)
            return out * inv_rms

        low_rank = total(0)
        z = offset[l : l + 1, :] + jnp.dot(
            jnp.tanh(low_rank[:, :rank]), decay_up[l], precision=lax.Precision.HIGHEST, preferred_element_type=F32
        )
        decay = to_rows(jnp.exp(sigmoid(z) * (-DECAY_SCALE) * pos[h * own : (h + 1) * own, :]), h, 0)
        learn = to_rows(
            sigmoid(
                jnp.dot(low_rank[:, rank:], rate_up[l], precision=lax.Precision.HIGHEST, preferred_element_type=F32)
            ),
            h,
            1,
        )
        keys = to_rows(total(1), h, 2)
        key_unit = keys * lax.rsqrt(half_sum(keys * keys) + 1.0)
        key_rate = key_unit * learn
        rows[h, 1] = key_rate
        query = to_rows(total(2), h, 3)
        key_query = half_sum(keys * query)
        rate_query = half_sum(key_rate * query)
        unit2 = twice(key_unit)
        query2 = twice(decay * query)
        if h == 0:
            loads[l, 5].wait()

        def products(t, acc):
            at = pl.ds(pl.multiple_of(t * TILE, TILE), TILE)
            s = state[l, h * count : (h + 1) * count, at]
            return (
                acc
                + jnp.dot((s * unit2).astype(BF16), gather1[at, :], preferred_element_type=F32)
                + jnp.dot((s * query2).astype(BF16), gather2[at, :], preferred_element_type=F32)
            )

        acc = lax.fori_loop(0, tiles, products, jnp.zeros((count, LANES), F32), unroll=True)
        turned = pltpu.roll(acc, HEAD, 1)
        state_key = jnp.where(low_rows, acc, turned)
        from_state = jnp.where(low_rows, turned, acc)
        value = to_rows(total(3), h, 4)
        readout = from_state - state_key * rate_query + value * key_query
        mean = half_sum(readout) * (1.0 / HEAD)
        centred = readout - mean
        var = half_sum(centred * centred) * (1.0 / HEAD)
        rows[h, 5] = centred * lax.rsqrt(var + GROUP_EPS)
        gate = sigmoid(total(4)) * head_gain[l : l + 1, :]
        normed = rows.at[h, 5]
        for j in range(width // LANES):
            even = normed[pl.ds(2 * j, own, stride=heads), :]
            odd = normed[pl.ds(2 * j + 1, own, stride=heads), :]
            cols = slice(j * LANES, (j + 1) * LANES)
            mixed_all[l, h, mine, cols] = (jnp.where(low, even, odd) * gate[:, cols]).astype(BF16)
        for o in range(1, n_dp):
            describe(
                ("ag", l, h, o),
                mixed_all.at[l, h, mine],
                mixed_all.at[l, h, mine],
                ag_send.at[l, h, o - 1],
                ag_recv.at[l, h, o - 1],
                {"dp": dp_peer(o)},
            ).start()

        def split(v):
            high = v.astype(BF16)
            rest = (v - high.astype(F32)).astype(BF16)
            return jnp.where(low_rows, high.astype(F32), rest.astype(F32)).astype(BF16)

        splits[h, 0] = split(value)
        splits[h, 1] = split(state_key)

    def update(l, h, first, last):
        def one(t, carry):
            at = pl.ds(pl.multiple_of(t * TILE, TILE), TILE)
            wide = jnp.dot(splits[h, 0], spread[:, at], preferred_element_type=F32)
            drop = jnp.dot(splits[h, 1], spread[:, at], preferred_element_type=F32)
            block = slice(h * count, (h + 1) * count)
            state[l, block, at] = (
                state[l, block, at] * twice(rows[h, 0]) - drop * twice(rows[h, 1]) + wide * twice(rows[h, 2])
            )
            return carry

        lax.fori_loop(first, last, one, 0, unroll=True)

    def output(l, h):
        for o in range(1, n_dp):
            copies["ag", l, h, o].wait_recv()
        if h == 0:
            loads[l, 6].wait()
        product = jnp.dot(mixed_all[l, h], wo[l], preferred_element_type=F32).astype(BF16)
        for k in range(reducers):
            i, j = k // strips, k % strips
            terms[l, h, k] = product[
                i * part_rows : (i + 1) * part_rows, j * part_cols : (j + 1) * part_cols
            ]
        for k in range(reducers):
            copy = describe(
                ("tr", l, h, k),
                terms.at[l, h, k],
                terms_got.at[l, h, lane_me],
                tr_send.at[l, h, k],
                tr_recv.at[l, h, lane_me],
                {"tp": first + k},
            )
            pl.when(lane_me != first + k)(copy.start)

    reducing = (lane_me >= first) & (lane_me < first + reducers)
    slot = jnp.clip(lane_me - first, 0, reducers - 1)

    def gather_terms(l, h):
        for o in range(1, n_tp):
            describe(
                ("ta", l, h, o),
                fresh.at[l, h, slot],
                fresh.at[l, h, slot],
                ta_send.at[l, h, o - 1],
                ta_recv.at[l, h, slot],
                {"tp": tp_peer(o)},
            )

        @pl.when(reducing)
        def _():
            acc = terms[l, h, slot].astype(F32)
            if l == 0:
                at_rows = pl.ds(pl.multiple_of(slot // strips * part_rows, part_rows), part_rows)
                at_cols = pl.ds(pl.multiple_of(slot % strips * part_cols, part_cols), part_cols)
                acc = acc + x_ref[h, at_rows, at_cols].astype(F32)
            else:
                acc = acc + fresh[l - 1, h, slot].astype(F32)
            for o in range(1, n_tp):
                there = tp_peer(o)
                pltpu.make_async_remote_copy(
                    src_ref=terms.at[l, h, slot],
                    dst_ref=terms_got.at[l, h, there],
                    send_sem=tr_send.at[l, h, slot],
                    recv_sem=tr_recv.at[l, h, there],
                    device_id={"tp": there},
                    device_id_type=MESH,
                ).wait_recv()
                acc = acc + terms_got[l, h, there].astype(F32)
            fresh[l, h, slot] = acc.astype(BF16)
            for o in range(1, n_tp):
                copies["ta", l, h, o].start()

    def renew(l, h):
        for k in range(reducers):
            copy = pltpu.make_async_remote_copy(
                src_ref=fresh.at[l, h, k],
                dst_ref=fresh.at[l, h, k],
                send_sem=ta_send.at[l, h, 0],
                recv_sem=ta_recv.at[l, h, k],
                device_id={"tp": tp_peer(1)},
                device_id_type=MESH,
            )
            pl.when(lane_me != first + k)(copy.wait_recv)

    def finish(h):
        for i in range(reducers // strips):
            strip = [fresh[BLOCK_COUNT - 1, h, i * strips + j] for j in range(strips)]
            value = jnp.concatenate(strip, axis=1)
            for d in range(n_dp):
                low_row, high_row = max(d * own, i * part_rows), min((d + 1) * own, (i + 1) * part_rows)
                if low_row < high_row:
                    to = d * (seq - own) + h * own
                    stream_out[to + low_row : to + high_row, :] = value[
                        low_row - i * part_rows : high_row - i * part_rows, :
                    ]

    every = range(halves)
    cut = [tiles * i // 2 for i in range(3)]
    project_all()
    lax.fori_loop(0, tiles, fill, 0)
    pos = prepare()
    for l in range(BLOCK_COUNT):
        if l > 0:
            for h in every:
                renew(l - 1, h)
                project(l, h)
        if l + 1 < BLOCK_COUNT:
            load_in(l + 1)
            load_rest(l + 1)
        for h in every:
            mix(l, h)
        for h in every:
            output(l, h)
            update(l, h, cut[0], cut[1])
        for h in every:
            gather_terms(l, h)
            update(l, h, cut[1], cut[2])
    for h in every:
        renew(BLOCK_COUNT - 1, h)
        finish(h)
    for key, copy in copies.items():
        if key[0] == "tr":
            pl.when(lane_me != first + key[3])(copy.wait_send)
        elif key[0] != "ta":
            copy.wait_send()

    @pl.when(reducing)
    def _():
        for key, copy in copies.items():
            if key[0] == "ta":
                copy.wait_send()


def flush(out, state, out_hbm, state_hbm, sem):
    copies = [pltpu.make_async_copy(out, out_hbm, sem.at[0])]
    for i in range(FLUSHES):
        rows = state.shape[1] // FLUSHES
        at = pl.ds(i * rows, rows)
        copies.append(pltpu.make_async_copy(state.at[:, at], state_hbm.at[:, at], sem.at[i + 1]))
    for copy in copies:
        copy.start()
    for copy in copies:
        copy.wait()


def solution(mesh):
    n_dp, n_tp = mesh.shape["dp"], mesh.shape["tp"]

    def body(
        stream,
        history,
        input_norm_gain,
        query_weight,
        key_weight,
        value_weight,
        gate_weight,
        adapter_down_weight,
        decay_up_weight,
        rate_up_weight,
        decay_offset,
        head_norm_gain,
        output_weight,
        recurrent_state,
    ):
        batch, depth = stream.shape
        width = query_weight.shape[2]
        blocks, seq, heads, vk = recurrent_state.shape
        count = seq * heads
        halves = PIECES if seq % (8 * PIECES) == 0 else 1
        span = batch // halves
        own = seq // halves
        lanes = (span + LANES - 1) // LANES * LANES
        reducers = n_tp // 2 if n_tp % 4 == 0 else n_tp
        strips = min(reducers, depth // LANES)
        part_rows, part_cols = span * strips // reducers, depth // strips
        columns = 4 * width + adapter_down_weight.shape[2]
        vmem = pl.BlockSpec(memory_space=pltpu.VMEM)
        hbm = pl.BlockSpec(memory_space=pl.ANY)
        dma = pltpu.SemaphoreType.DMA

        def like(w):
            return pltpu.VMEM(w.shape, w.dtype)

        out, new_state = pl.pallas_call(
            functools.partial(kernel, n_dp, n_tp, halves),
            out_shape=(
                pltpu.VMEM((batch, depth), BF16),
                pltpu.VMEM((blocks, count, vk), F32),
            ),
            in_specs=[hbm] * 14,
            out_specs=(vmem, vmem),
            scratch_shapes=[
                like(stream),
                pltpu.VMEM((1, seq), history.dtype),
                like(input_norm_gain),
                like(decay_up_weight),
                like(rate_up_weight),
                like(decay_offset),
                like(head_norm_gain),
                like(adapter_down_weight),
                like(key_weight),
                like(query_weight),
                like(value_weight),
                like(gate_weight),
                like(output_weight),
                pltpu.VMEM((blocks, halves, span, columns), BF16),
                pltpu.VMEM((blocks, halves, n_dp - 1, own, columns), BF16),
                pltpu.VMEM((blocks, halves, 8, lanes), F32),
                pltpu.VMEM((blocks, halves, n_dp - 1, 8, lanes), F32),
                pltpu.VMEM((blocks, halves, span, width), BF16),
                pltpu.VMEM((blocks, halves, reducers, part_rows, part_cols), BF16),
                pltpu.VMEM((blocks, halves, n_tp, part_rows, part_cols), BF16),
                pltpu.VMEM((blocks, halves, reducers, part_rows, part_cols), BF16),
                pltpu.VMEM((halves, span, depth), BF16),
                pltpu.VMEM((halves, 6, count // halves, LANES), F32),
                pltpu.VMEM((halves, 2, count // halves, LANES), BF16),
                pltpu.VMEM((vk, LANES), BF16),
                pltpu.VMEM((vk, LANES), BF16),
                pltpu.VMEM((LANES, vk), BF16),
                dma((7,)),
                dma((blocks, 7)),
                dma((blocks, halves, 5, n_dp - 1)),
                dma((blocks, halves, 5, n_dp - 1)),
                dma((blocks, halves, n_dp - 1)),
                dma((blocks, halves, n_dp - 1)),
                dma((blocks, halves, n_dp - 1)),
                dma((blocks, halves, n_dp - 1)),
                dma((blocks, halves, reducers)),
                dma((blocks, halves, n_tp)),
                dma((blocks, halves, n_tp - 1)),
                dma((blocks, halves, reducers)),
            ],
            compiler_params=pltpu.CompilerParams(
                collective_id=0, has_side_effects=True, vmem_limit_bytes=54 * 1024 * 1024
            ),
        )(
            stream,
            history[None, :],
            input_norm_gain,
            adapter_down_weight,
            key_weight,
            query_weight,
            value_weight,
            gate_weight,
            decay_up_weight,
            rate_up_weight,
            decay_offset,
            head_norm_gain,
            output_weight,
            recurrent_state.reshape(blocks, count, vk),
        )
        out, new_state = pl.pallas_call(
            flush,
            out_shape=(
                jax.ShapeDtypeStruct((batch, depth), BF16),
                jax.ShapeDtypeStruct((blocks, count, vk), F32),
            ),
            in_specs=[hbm, hbm],
            out_specs=(hbm, hbm),
            scratch_shapes=[dma((FLUSHES + 1,))],
            compiler_params=pltpu.CompilerParams(vmem_limit_bytes=1024 * 1024),
        )(out, new_state)
        return out, new_state.reshape(blocks, seq, heads, vk)

    placed = (
        P(None, "dp"),
        P("dp"),
        P(None, "dp"),
        P(None, "dp", "tp"),
        P(None, "dp", "tp"),
        P(None, "dp", "tp"),
        P(None, "dp", "tp"),
        P(None, "dp", None),
        P(None, None, "tp"),
        P(None, None, "tp"),
        P(None, "tp"),
        P(None, "tp"),
        P(None, "tp", "dp"),
        P(None, "dp", "tp", None),
    )
    return jax.shard_map(
        body,
        mesh=mesh,
        in_specs=placed,
        out_specs=(P(None, "dp"), P(None, "dp", "tp", None)),
        check_vma=False,
    )
```

```python
import functools

import jax
import jax.numpy as jnp
from jax import lax
from jax.experimental import pallas as pl
from jax.experimental.pallas import tpu as pltpu
from jax.sharding import PartitionSpec as P

HEAD = 64
SPAN = 64
BLOCK_COUNT = 2
LANES = 128
NORM_EPS = 0.25
GROUP_EPS = 0.25
DECAY_SCALE = 0.6065306597126334
TILE = 256
FLUSHES = 8
PIECES = 2
GROUPS = ((0,), (1,), (2,), (3,), (4,))
MESH = pl.DeviceIdType.MESH
F32 = jnp.float32
BF16 = jnp.bfloat16


def sigmoid(z):
    e = jnp.exp(-jnp.abs(z))
    return jnp.where(z >= 0, 1.0, e) / (1.0 + e)


def kernel(
    n_dp,
    n_tp,
    halves,
    stream_hbm,
    history_hbm,
    in_gain_hbm,
    adapter_hbm,
    key_hbm,
    query_hbm,
    value_hbm,
    gate_hbm,
    decay_up_hbm,
    rate_up_hbm,
    offset_hbm,
    head_gain_hbm,
    out_hbm,
    state_hbm,
    stream_out,
    state,
    stream_ref,
    history_ref,
    in_gain,
    decay_up,
    rate_up,
    offset,
    head_gain,
    wa,
    wk,
    wq,
    wv,
    wg,
    wo,
    sent,
    got,
    sq_sent,
    sq_got,
    mixed_all,
    terms,
    terms_got,
    fresh,
    x_ref,
    rows,
    splits,
    gather1,
    gather2,
    spread,
    small_sem,
    load_sem,
    rs_send,
    rs_recv,
    sq_send,
    sq_recv,
    ag_send,
    ag_recv,
    tr_send,
    tr_recv,
    ta_send,
    ta_recv,
):
    me = lax.axis_index("dp")
    lane_me = lax.axis_index("tp")
    batch, depth = stream_ref.shape
    seq = batch // n_dp
    width = wk.shape[2]
    heads = width // HEAD
    span = batch // halves
    own = seq // halves
    count = own * heads
    rank = wa.shape[2] // 2
    vk = state.shape[2]
    tiles = vk // TILE
    lanes = sq_sent.shape[3]
    reducers, part_rows, part_cols = terms.shape[2:]
    first = (n_tp - reducers) // 2
    strips = depth // part_cols

    def dp_peer(o):
        return lax.rem(me + o, n_dp)

    def tp_peer(o):
        return lax.rem(lane_me + o, n_tp)

    barrier = pltpu.get_barrier_semaphore()
    for o in range(1, n_tp):
        pl.semaphore_signal(barrier, inc=1, device_id={"tp": tp_peer(o)}, device_id_type=MESH)
    for o in range(1, n_dp):
        pl.semaphore_signal(barrier, inc=1, device_id={"dp": dp_peer(o)}, device_id_type=MESH)

    loads = {}
    small = []

    def load(l, i, src, dst):
        loads[l, i] = pltpu.make_async_copy(src.at[l], dst.at[l], load_sem.at[l, i])
        loads[l, i].start()

    def load_small(src, dst):
        small.append(pltpu.make_async_copy(src, dst, small_sem.at[len(small)]))
        small[-1].start()

    def load_in(l):
        load(l, 0, adapter_hbm, wa)
        load(l, 1, key_hbm, wk)
        load(l, 2, query_hbm, wq)
        load(l, 3, value_hbm, wv)
        load(l, 4, gate_hbm, wg)

    def load_rest(l):
        load(l, 5, state_hbm, state)
        load(l, 6, out_hbm, wo)

    load_small(stream_hbm, stream_ref)
    load_small(in_gain_hbm, in_gain)
    load_in(0)
    load_small(history_hbm, history_ref)
    load_small(decay_up_hbm, decay_up)
    load_small(rate_up_hbm, rate_up)
    load_small(offset_hbm, offset)
    load_small(head_gain_hbm, head_gain)
    load_rest(0)

    def fill(t, carry):
        at = pl.ds(pl.multiple_of(t * TILE, TILE), TILE)
        r = (lax.broadcasted_iota(jnp.int32, (TILE, LANES), 0) + t * TILE) // HEAD
        c = lax.broadcasted_iota(jnp.int32, (TILE, LANES), 1)
        gather1[at, :] = jnp.where(r == c, 1.0, 0.0).astype(BF16)
        gather2[at, :] = jnp.where(r + HEAD == c, 1.0, 0.0).astype(BF16)
        r = lax.broadcasted_iota(jnp.int32, (LANES, TILE), 0)
        c = (lax.broadcasted_iota(jnp.int32, (LANES, TILE), 1) + t * TILE) // HEAD
        spread[:, at] = jnp.where((r == c) | (r == c + HEAD), 1.0, 0.0).astype(BF16)
        return carry

    low = lax.broadcasted_iota(jnp.int32, (own, LANES), 1) < HEAD
    low_rows = lax.broadcasted_iota(jnp.int32, (count, LANES), 1) < HEAD

    def to_rows(value, h, i):
        buf = rows.at[h, i]
        for j in range(width // LANES):
            pair = value[:, j * LANES : (j + 1) * LANES]
            turned = pltpu.roll(pair, HEAD, 1)
            buf[pl.ds(2 * j, own, stride=heads), :] = jnp.where(low, pair, turned)
            buf[pl.ds(2 * j + 1, own, stride=heads), :] = jnp.where(low, turned, pair)
        return rows[h, i]

    def half_sum(v):
        return jnp.sum(v, axis=1, keepdims=True) * 0.5

    def twice(v):
        return jnp.concatenate([v, v], axis=1)

    mine = pl.ds(pl.multiple_of(me * own, own), own)
    row_at = lax.broadcasted_iota(jnp.int32, (span, lanes), 0)
    diag = row_at == lax.broadcasted_iota(jnp.int32, (span, lanes), 1)
    own_at = lax.broadcasted_iota(jnp.int32, (own, lanes), 0) + me * own
    own_diag = own_at == lax.broadcasted_iota(jnp.int32, (own, lanes), 1)
    sizes = [2 * rank, width, width, width, width]
    starts = [sum(sizes[:c]) for c in range(5)]
    def copy_of(src, dst, send, recv, where):
        return pltpu.make_async_remote_copy(
            src_ref=src, dst_ref=dst, send_sem=send, recv_sem=recv, device_id=where, device_id_type=MESH
        )

    def arrived(ref, recv):
        copy_of(ref, ref, tr_send, recv, {"tp": tp_peer(1)}).wait_recv()

    def left(ref, send):
        copy_of(ref, ref, send, ta_recv.at[0, 0], {"tp": tp_peer(1)}).wait_send()

    def send_squares(l, h):
        for o in range(1, n_dp):
            copy_of(sq_sent.at[l, h], sq_got.at[l, h, o - 1], sq_send, sq_recv.at[l, h], {"dp": dp_peer(o)}).start()

    def columns_of(g):
        return pl.ds(starts[GROUPS[g][0]], sum(sizes[c] for c in GROUPS[g]))

    def send_columns(l, h, g):
        cols = columns_of(g)
        for o in range(1, n_dp):
            there = dp_peer(o)
            at = pl.ds(pl.multiple_of(there * own, own), own)
            copy_of(
                sent.at[l, h, at, cols], got.at[l, h, o - 1, :, cols], rs_send, rs_recv.at[l, h, g], {"dp": there}
            ).start()

    def put_squares(l, h, x):
        column = jnp.sum(x * x, axis=1, keepdims=True)
        line = jnp.sum(jnp.where(diag, column, 0.0), axis=0, keepdims=True)
        sq_sent[l, h] = jnp.broadcast_to(line, (8, lanes))

    weights = (wa, wk, wq, wv, wg)

    def project_all():
        small[0].wait()
        small[1].wait()
        for h in range(halves):
            for d in range(n_dp):
                x_ref[h, d * own : (d + 1) * own, :] = stream_ref[
                    d * seq + h * own : d * seq + (h + 1) * own, :
                ]
        for h in range(halves):
            put_squares(0, h, x_ref[h].astype(F32))
        x = x_ref[...].reshape(batch, depth).astype(F32)
        scaled = (x * in_gain[:1, :]).astype(BF16)
        for c, weight in enumerate(weights):
            loads[0, c].wait()
            cols = pl.ds(starts[c], sizes[c])
            product = jnp.dot(scaled, weight[0], preferred_element_type=F32).astype(BF16)
            sent[0, :, :, cols] = product.reshape(halves, span, sizes[c])
        pl.semaphore_wait(barrier, n_dp + n_tp - 2)
        for h in range(halves):
            send_squares(0, h)
            for g in range(len(GROUPS)):
                send_columns(0, h, g)

    def project(l, h):
        rows_of = []
        for i in range(reducers // strips):
            strip = [fresh[l - 1, h, i * strips + j] for j in range(strips)]
            rows_of.append(jnp.concatenate(strip, axis=1))
        x = jnp.concatenate(rows_of, axis=0).astype(F32)
        put_squares(l, h, x)
        scaled = (x * in_gain[l : l + 1, :]).astype(BF16)
        send_squares(l, h)
        for c, weight in enumerate(weights):
            if h == 0:
                loads[l, c].wait()
            cols = pl.ds(starts[c], sizes[c])
            sent[l, h, :, cols] = jnp.dot(scaled, weight[l], preferred_element_type=F32).astype(BF16)
            for g in range(len(GROUPS)):
                if GROUPS[g][-1] == c:
                    send_columns(l, h, g)

    def prepare():
        for copy in small[2:]:
            copy.wait()
        spans = jnp.floor(history_ref[...].astype(F32) * (1.0 / SPAN))
        phase = 0.5 + (spans - 3.0 * jnp.floor((spans + 0.5) * (1.0 / 3.0)))
        diagonal = lax.broadcasted_iota(jnp.int32, (seq, seq), 0) == lax.broadcasted_iota(jnp.int32, (seq, seq), 1)
        return jnp.sum(jnp.where(diagonal, phase, 0.0), axis=1, keepdims=True)

    def mix(l, h):
        arrived(sq_got.at[l, h], sq_recv.at[l, h])
        line = sq_sent[l, h]
        for o in range(1, n_dp):
            line = line + sq_got[l, h, o - 1]
        squares = jnp.sum(jnp.where(own_diag, line[:1, :], 0.0), axis=1, keepdims=True)
        inv_rms = lax.rsqrt(squares / (depth * n_dp) + NORM_EPS)

        def total(c):
            for g in range(len(GROUPS)):
                if GROUPS[g][0] == c:
                    arrived(got.at[l, h, :, :, columns_of(g)], rs_recv.at[l, h, g])
            cols = pl.ds(starts[c], sizes[c])
            out = sent[l, h, mine, cols].astype(F32)
            for o in range(1, n_dp):
                out = out + got[l, h, o - 1, :, cols].astype(F32)
            return out * inv_rms

        low_rank = total(0)
        z = offset[l : l + 1, :] + jnp.dot(
            jnp.tanh(low_rank[:, :rank]), decay_up[l], precision=lax.Precision.HIGHEST, preferred_element_type=F32
        )
        decay = to_rows(jnp.exp(sigmoid(z) * (-DECAY_SCALE) * pos[h * own : (h + 1) * own, :]), h, 0)
        learn = to_rows(
            sigmoid(
                jnp.dot(low_rank[:, rank:], rate_up[l], precision=lax.Precision.HIGHEST, preferred_element_type=F32)
            ),
            h,
            1,
        )
        keys = to_rows(total(1), h, 2)
        key_unit = keys * lax.rsqrt(half_sum(keys * keys) + 1.0)
        key_rate = key_unit * learn
        rows[h, 1] = key_rate
        query = to_rows(total(2), h, 3)
        key_query = half_sum(keys * query)
        rate_query = half_sum(key_rate * query)
        unit2 = twice(key_unit)
        query2 = twice(decay * query)
        if h == 0:
            loads[l, 5].wait()

        def products(t, acc):
            at = pl.ds(pl.multiple_of(t * TILE, TILE), TILE)
            s = state[l, h * count : (h + 1) * count, at]
            return (
                acc
                + jnp.dot((s * unit2).astype(BF16), gather1[at, :], preferred_element_type=F32)
                + jnp.dot((s * query2).astype(BF16), gather2[at, :], preferred_element_type=F32)
            )

        acc = lax.fori_loop(0, tiles, products, jnp.zeros((count, LANES), F32), unroll=True)
        turned = pltpu.roll(acc, HEAD, 1)
        state_key = jnp.where(low_rows, acc, turned)
        from_state = jnp.where(low_rows, turned, acc)
        value = to_rows(total(3), h, 4)
        readout = from_state - state_key * rate_query + value * key_query
        mean = half_sum(readout) * (1.0 / HEAD)
        centred = readout - mean
        var = half_sum(centred * centred) * (1.0 / HEAD)
        rows[h, 5] = centred * lax.rsqrt(var + GROUP_EPS)
        gate = sigmoid(total(4)) * head_gain[l : l + 1, :]
        normed = rows.at[h, 5]
        for j in range(width // LANES):
            even = normed[pl.ds(2 * j, own, stride=heads), :]
            odd = normed[pl.ds(2 * j + 1, own, stride=heads), :]
            cols = slice(j * LANES, (j + 1) * LANES)
            mixed_all[l, h, mine, cols] = (jnp.where(low, even, odd) * gate[:, cols]).astype(BF16)
        for o in range(1, n_dp):
            copy_of(
                mixed_all.at[l, h, mine], mixed_all.at[l, h, mine], ag_send, ag_recv.at[l, h], {"dp": dp_peer(o)}
            ).start()

        def split(v):
            high = v.astype(BF16)
            rest = (v - high.astype(F32)).astype(BF16)
            return jnp.where(low_rows, high.astype(F32), rest.astype(F32)).astype(BF16)

        splits[h, 0] = split(value)
        splits[h, 1] = split(state_key)

    def update(l, h, first, last):
        def one(t, carry):
            at = pl.ds(pl.multiple_of(t * TILE, TILE), TILE)
            wide = jnp.dot(splits[h, 0], spread[:, at], preferred_element_type=F32)
            drop = jnp.dot(splits[h, 1], spread[:, at], preferred_element_type=F32)
            block = slice(h * count, (h + 1) * count)
            state[l, block, at] = (
                state[l, block, at] * twice(rows[h, 0]) - drop * twice(rows[h, 1]) + wide * twice(rows[h, 2])
            )
            return carry

        lax.fori_loop(first, last, one, 0, unroll=True)

    def output(l, h):
        arrived(mixed_all.at[l, h, : (n_dp - 1) * own], ag_recv.at[l, h])
        if h == 0:
            loads[l, 6].wait()
        product = jnp.dot(mixed_all[l, h], wo[l], preferred_element_type=F32).astype(BF16)
        for k in range(reducers):
            i, j = k // strips, k % strips
            terms[l, h, k] = product[
                i * part_rows : (i + 1) * part_rows, j * part_cols : (j + 1) * part_cols
            ]
        for k in range(reducers):
            copy = copy_of(
                terms.at[l, h, k], terms_got.at[l, h, lane_me], tr_send, tr_recv.at[l, h], {"tp": first + k}
            )
            pl.when(lane_me != first + k)(copy.start)

    reducing = (lane_me >= first) & (lane_me < first + reducers)
    slot = jnp.clip(lane_me - first, 0, reducers - 1)

    def gather_terms(l, h):
        @pl.when(reducing)
        def _():
            acc = terms[l, h, slot].astype(F32)
            if l == 0:
                at_rows = pl.ds(pl.multiple_of(slot // strips * part_rows, part_rows), part_rows)
                at_cols = pl.ds(pl.multiple_of(slot % strips * part_cols, part_cols), part_cols)
                acc = acc + x_ref[h, at_rows, at_cols].astype(F32)
            else:
                acc = acc + fresh[l - 1, h, slot].astype(F32)
            arrived(terms_got.at[l, h, : n_tp - 1], tr_recv.at[l, h])
            for o in range(1, n_tp):
                acc = acc + terms_got[l, h, tp_peer(o)].astype(F32)
            fresh[l, h, slot] = acc.astype(BF16)
            for o in range(1, n_tp):
                copy_of(
                    fresh.at[l, h, slot], fresh.at[l, h, slot], ta_send, ta_recv.at[l, h], {"tp": tp_peer(o)}
                ).start()

    def renew(l, h):
        @pl.when(reducing)
        def _():
            arrived(fresh.at[l, h, : reducers - 1], ta_recv.at[l, h])

        if reducers < n_tp:

            @pl.when(jnp.logical_not(reducing))
            def _():
                arrived(fresh.at[l, h], ta_recv.at[l, h])

    def finish(h):
        for i in range(reducers // strips):
            strip = [fresh[BLOCK_COUNT - 1, h, i * strips + j] for j in range(strips)]
            value = jnp.concatenate(strip, axis=1)
            for d in range(n_dp):
                low_row, high_row = max(d * own, i * part_rows), min((d + 1) * own, (i + 1) * part_rows)
                if low_row < high_row:
                    to = d * (seq - own) + h * own
                    stream_out[to + low_row : to + high_row, :] = value[
                        low_row - i * part_rows : high_row - i * part_rows, :
                    ]

    every = range(halves)
    cut = [tiles * i // 2 for i in range(3)]
    project_all()
    lax.fori_loop(0, tiles, fill, 0)
    pos = prepare()
    for l in range(BLOCK_COUNT):
        if l > 0:
            for h in every:
                renew(l - 1, h)
                project(l, h)
        if l + 1 < BLOCK_COUNT:
            load_in(l + 1)
            load_rest(l + 1)
        for h in every:
            mix(l, h)
        for h in every:
            output(l, h)
            update(l, h, cut[0], cut[1])
        for h in every:
            gather_terms(l, h)
            update(l, h, cut[1], cut[2])
    for h in every:
        renew(BLOCK_COUNT - 1, h)
        finish(h)
    left(got, rs_send)
    left(sq_got, sq_send)
    left(mixed_all.at[:, :, : (n_dp - 1) * own], ag_send)

    @pl.when(reducing)
    def _():
        left(terms.at[:, :, : reducers - 1], tr_send)
        left(terms_got.at[:, :, : n_tp - 1], ta_send)

    if reducers < n_tp:

        @pl.when(jnp.logical_not(reducing))
        def _():
            left(terms, tr_send)


def flush(out, state, out_hbm, state_hbm, sem):
    copies = [pltpu.make_async_copy(out, out_hbm, sem.at[0])]
    for i in range(FLUSHES):
        rows = state.shape[1] // FLUSHES
        at = pl.ds(i * rows, rows)
        copies.append(pltpu.make_async_copy(state.at[:, at], state_hbm.at[:, at], sem.at[i + 1]))
    for copy in copies:
        copy.start()
    for copy in copies:
        copy.wait()


def solution(mesh):
    n_dp, n_tp = mesh.shape["dp"], mesh.shape["tp"]

    def body(
        stream,
        history,
        input_norm_gain,
        query_weight,
        key_weight,
        value_weight,
        gate_weight,
        adapter_down_weight,
        decay_up_weight,
        rate_up_weight,
        decay_offset,
        head_norm_gain,
        output_weight,
        recurrent_state,
    ):
        batch, depth = stream.shape
        width = query_weight.shape[2]
        blocks, seq, heads, vk = recurrent_state.shape
        count = seq * heads
        halves = PIECES if seq % (8 * PIECES) == 0 else 1
        span = batch // halves
        own = seq // halves
        lanes = (span + LANES - 1) // LANES * LANES
        reducers = n_tp // 2 if n_tp % 4 == 0 else n_tp
        strips = min(reducers, depth // LANES)
        part_rows, part_cols = span * strips // reducers, depth // strips
        columns = 4 * width + adapter_down_weight.shape[2]
        vmem = pl.BlockSpec(memory_space=pltpu.VMEM)
        hbm = pl.BlockSpec(memory_space=pl.ANY)
        dma = pltpu.SemaphoreType.DMA

        def like(w):
            return pltpu.VMEM(w.shape, w.dtype)

        out, new_state = pl.pallas_call(
            functools.partial(kernel, n_dp, n_tp, halves),
            out_shape=(
                pltpu.VMEM((batch, depth), BF16),
                pltpu.VMEM((blocks, count, vk), F32),
            ),
            in_specs=[hbm] * 14,
            out_specs=(vmem, vmem),
            scratch_shapes=[
                like(stream),
                pltpu.VMEM((1, seq), history.dtype),
                like(input_norm_gain),
                like(decay_up_weight),
                like(rate_up_weight),
                like(decay_offset),
                like(head_norm_gain),
                like(adapter_down_weight),
                like(key_weight),
                like(query_weight),
                like(value_weight),
                like(gate_weight),
                like(output_weight),
                pltpu.VMEM((blocks, halves, span, columns), BF16),
                pltpu.VMEM((blocks, halves, n_dp - 1, own, columns), BF16),
                pltpu.VMEM((blocks, halves, 8, lanes), F32),
                pltpu.VMEM((blocks, halves, n_dp - 1, 8, lanes), F32),
                pltpu.VMEM((blocks, halves, span, width), BF16),
                pltpu.VMEM((blocks, halves, reducers, part_rows, part_cols), BF16),
                pltpu.VMEM((blocks, halves, n_tp, part_rows, part_cols), BF16),
                pltpu.VMEM((blocks, halves, reducers, part_rows, part_cols), BF16),
                pltpu.VMEM((halves, span, depth), BF16),
                pltpu.VMEM((halves, 6, count // halves, LANES), F32),
                pltpu.VMEM((halves, 2, count // halves, LANES), BF16),
                pltpu.VMEM((vk, LANES), BF16),
                pltpu.VMEM((vk, LANES), BF16),
                pltpu.VMEM((LANES, vk), BF16),
                dma((7,)),
                dma((blocks, 7)),
                dma,
                dma((blocks, halves, len(GROUPS))),
                dma,
                dma((blocks, halves)),
                dma,
                dma((blocks, halves)),
                dma,
                dma((blocks, halves)),
                dma,
                dma((blocks, halves)),
            ],
            compiler_params=pltpu.CompilerParams(
                collective_id=0, has_side_effects=True, vmem_limit_bytes=54 * 1024 * 1024
            ),
        )(
            stream,
            history[None, :],
            input_norm_gain,
            adapter_down_weight,
            key_weight,
            query_weight,
            value_weight,
            gate_weight,
            decay_up_weight,
            rate_up_weight,
            decay_offset,
            head_norm_gain,
            output_weight,
            recurrent_state.reshape(blocks, count, vk),
        )
        out, new_state = pl.pallas_call(
            flush,
            out_shape=(
                jax.ShapeDtypeStruct((batch, depth), BF16),
                jax.ShapeDtypeStruct((blocks, count, vk), F32),
            ),
            in_specs=[hbm, hbm],
            out_specs=(hbm, hbm),
            scratch_shapes=[dma((FLUSHES + 1,))],
            compiler_params=pltpu.CompilerParams(vmem_limit_bytes=1024 * 1024),
        )(out, new_state)
        return out, new_state.reshape(blocks, seq, heads, vk)

    placed = (
        P(None, "dp"),
        P("dp"),
        P(None, "dp"),
        P(None, "dp", "tp"),
        P(None, "dp", "tp"),
        P(None, "dp", "tp"),
        P(None, "dp", "tp"),
        P(None, "dp", None),
        P(None, None, "tp"),
        P(None, None, "tp"),
        P(None, "tp"),
        P(None, "tp"),
        P(None, "tp", "dp"),
        P(None, "dp", "tp", None),
    )
    return jax.shard_map(
        body,
        mesh=mesh,
        in_specs=placed,
        out_specs=(P(None, "dp"), P(None, "dp", "tp", None)),
        check_vma=False,
    )
```

```python
import functools

import jax
import jax.numpy as jnp
from jax import lax
from jax.experimental import pallas as pl
from jax.experimental.pallas import tpu as pltpu
from jax.sharding import PartitionSpec as P

HEAD = 64
SPAN = 64
BLOCK_COUNT = 2
LANES = 128
NORM_EPS = 0.25
GROUP_EPS = 0.25
DECAY_SCALE = 0.6065306597126334
TILE = 256
FLUSHES = 8
PIECES = 2
GROUPS = ((0,), (1,), (2,), (3,), (4,))
MESH = pl.DeviceIdType.MESH
F32 = jnp.float32
BF16 = jnp.bfloat16


def sigmoid(z):
    e = jnp.exp(-jnp.abs(z))
    return jnp.where(z >= 0, 1.0, e) / (1.0 + e)


def kernel(
    n_dp,
    n_tp,
    halves,
    stream_hbm,
    history_hbm,
    in_gain_hbm,
    adapter_hbm,
    key_hbm,
    query_hbm,
    value_hbm,
    gate_hbm,
    decay_up_hbm,
    rate_up_hbm,
    offset_hbm,
    head_gain_hbm,
    out_hbm,
    state_hbm,
    stream_out,
    state,
    stream_ref,
    history_ref,
    in_gain,
    decay_up,
    rate_up,
    offset,
    head_gain,
    wa,
    wk,
    wq,
    wv,
    wg,
    wo,
    sent,
    got,
    sq_sent,
    sq_got,
    mixed_all,
    terms,
    terms_got,
    fresh,
    x_ref,
    rows,
    splits,
    gather1,
    gather2,
    spread,
    small_sem,
    load_sem,
    rs_send,
    rs_recv,
    sq_send,
    sq_recv,
    ag_send,
    ag_recv,
    tr_send,
    tr_recv,
    ta_send,
    ta_recv,
):
    me = lax.axis_index("dp")
    lane_me = lax.axis_index("tp")
    batch, depth = stream_ref.shape
    seq = batch // n_dp
    width = wk.shape[2]
    heads = width // HEAD
    span = batch // halves
    own = seq // halves
    count = own * heads
    rank = wa.shape[2] // 2
    vk = state.shape[2]
    tiles = vk // TILE
    lanes = sq_sent.shape[3]
    reducers, part_rows, part_cols = terms.shape[2:]
    first = (n_tp - reducers) // 2
    strips = depth // part_cols

    def dp_peer(o):
        return lax.rem(me + o, n_dp)

    def tp_peer(o):
        return lax.rem(lane_me + o, n_tp)

    barrier = pltpu.get_barrier_semaphore()
    for o in range(1, n_tp):
        pl.semaphore_signal(barrier, inc=1, device_id={"tp": tp_peer(o)}, device_id_type=MESH)
    for o in range(1, n_dp):
        pl.semaphore_signal(barrier, inc=1, device_id={"dp": dp_peer(o)}, device_id_type=MESH)

    loads = {}
    small = []

    def load(l, i, src, dst):
        loads[l, i] = pltpu.make_async_copy(src.at[l], dst.at[l], load_sem.at[l, i])
        loads[l, i].start()

    def load_small(src, dst):
        small.append(pltpu.make_async_copy(src, dst, small_sem.at[len(small)]))
        small[-1].start()

    def load_in(l):
        load(l, 0, adapter_hbm, wa)
        load(l, 1, key_hbm, wk)
        load(l, 2, query_hbm, wq)
        load(l, 3, value_hbm, wv)
        load(l, 4, gate_hbm, wg)

    def load_rest(l):
        load(l, 5, state_hbm, state)
        load(l, 6, out_hbm, wo)

    load_small(stream_hbm, stream_ref)
    load_small(in_gain_hbm, in_gain)
    load_in(0)
    load_small(history_hbm, history_ref)
    load_small(decay_up_hbm, decay_up)
    load_small(rate_up_hbm, rate_up)
    load_small(offset_hbm, offset)
    load_small(head_gain_hbm, head_gain)
    load_rest(0)

    def fill(t, carry):
        at = pl.ds(pl.multiple_of(t * TILE, TILE), TILE)
        r = (lax.broadcasted_iota(jnp.int32, (TILE, LANES), 0) + t * TILE) // HEAD
        c = lax.broadcasted_iota(jnp.int32, (TILE, LANES), 1)
        gather1[at, :] = jnp.where(r == c, 1.0, 0.0).astype(BF16)
        gather2[at, :] = jnp.where(r + HEAD == c, 1.0, 0.0).astype(BF16)
        r = lax.broadcasted_iota(jnp.int32, (LANES, TILE), 0)
        c = (lax.broadcasted_iota(jnp.int32, (LANES, TILE), 1) + t * TILE) // HEAD
        spread[:, at] = jnp.where((r == c) | (r == c + HEAD), 1.0, 0.0).astype(BF16)
        return carry

    low = lax.broadcasted_iota(jnp.int32, (own, LANES), 1) < HEAD
    low_rows = lax.broadcasted_iota(jnp.int32, (count, LANES), 1) < HEAD

    def to_rows(value, h, i):
        buf = rows.at[h, i]
        for j in range(width // LANES):
            pair = value[:, j * LANES : (j + 1) * LANES]
            turned = pltpu.roll(pair, HEAD, 1)
            buf[pl.ds(2 * j, own, stride=heads), :] = jnp.where(low, pair, turned)
            buf[pl.ds(2 * j + 1, own, stride=heads), :] = jnp.where(low, turned, pair)
        return rows[h, i]

    def half_sum(v):
        return jnp.sum(v, axis=1, keepdims=True) * 0.5

    def twice(v):
        return jnp.concatenate([v, v], axis=1)

    mine = pl.ds(pl.multiple_of(me * own, own), own)
    row_at = lax.broadcasted_iota(jnp.int32, (span, lanes), 0)
    diag = row_at == lax.broadcasted_iota(jnp.int32, (span, lanes), 1)
    own_at = lax.broadcasted_iota(jnp.int32, (own, lanes), 0) + me * own
    own_diag = own_at == lax.broadcasted_iota(jnp.int32, (own, lanes), 1)
    sizes = [2 * rank, width, width, width, width]
    starts = [sum(sizes[:c]) for c in range(5)]
    def copy_of(src, dst, send, recv, where):
        return pltpu.make_async_remote_copy(
            src_ref=src, dst_ref=dst, send_sem=send, recv_sem=recv, device_id=where, device_id_type=MESH
        )

    def arrived(ref, recv):
        copy_of(ref, ref, tr_send, recv, {"tp": tp_peer(1)}).wait_recv()

    def left(ref, send):
        copy_of(ref, ref, send, ta_recv.at[0, 0], {"tp": tp_peer(1)}).wait_send()

    def send_squares(l, h):
        for o in range(1, n_dp):
            copy_of(sq_sent.at[l, h], sq_got.at[l, h, o - 1], sq_send, sq_recv.at[l, h], {"dp": dp_peer(o)}).start()

    def columns_of(g):
        return pl.ds(starts[GROUPS[g][0]], sum(sizes[c] for c in GROUPS[g]))

    def send_columns(l, h, g):
        cols = columns_of(g)
        for o in range(1, n_dp):
            there = dp_peer(o)
            at = pl.ds(pl.multiple_of(there * own, own), own)
            copy_of(
                sent.at[l, h, at, cols], got.at[l, h, o - 1, :, cols], rs_send, rs_recv.at[l, h, g], {"dp": there}
            ).start()

    def put_squares(l, h, x):
        column = jnp.sum(x * x, axis=1, keepdims=True)
        line = jnp.sum(jnp.where(diag, column, 0.0), axis=0, keepdims=True)
        sq_sent[l, h] = jnp.broadcast_to(line, (8, lanes))

    weights = (wa, wk, wq, wv, wg)

    def project_all():
        small[0].wait()
        small[1].wait()
        for h in range(halves):
            for d in range(n_dp):
                x_ref[h, d * own : (d + 1) * own, :] = stream_ref[
                    d * seq + h * own : d * seq + (h + 1) * own, :
                ]
        for h in range(halves):
            put_squares(0, h, x_ref[h].astype(F32))
        x = x_ref[...].reshape(batch, depth).astype(F32)
        scaled = (x * in_gain[:1, :]).astype(BF16)
        for c, weight in enumerate(weights):
            loads[0, c].wait()
            cols = pl.ds(starts[c], sizes[c])
            product = jnp.dot(scaled, weight[0], preferred_element_type=F32).astype(BF16)
            sent[0, :, :, cols] = product.reshape(halves, span, sizes[c])
        pl.semaphore_wait(barrier, n_dp + n_tp - 2)
        for h in range(halves):
            send_squares(0, h)
            for g in range(len(GROUPS)):
                send_columns(0, h, g)

    def project(l, h):
        rows_of = []
        for i in range(reducers // strips):
            strip = [fresh[l - 1, h, i * strips + j] for j in range(strips)]
            rows_of.append(jnp.concatenate(strip, axis=1))
        x = jnp.concatenate(rows_of, axis=0).astype(F32)
        put_squares(l, h, x)
        scaled = (x * in_gain[l : l + 1, :]).astype(BF16)
        send_squares(l, h)
        for c, weight in enumerate(weights):
            if h == 0:
                loads[l, c].wait()
            cols = pl.ds(starts[c], sizes[c])
            sent[l, h, :, cols] = jnp.dot(scaled, weight[l], preferred_element_type=F32).astype(BF16)
            for g in range(len(GROUPS)):
                if GROUPS[g][-1] == c:
                    send_columns(l, h, g)

    def prepare():
        for copy in small[2:]:
            copy.wait()
        spans = jnp.floor(history_ref[...].astype(F32) * (1.0 / SPAN))
        phase = 0.5 + (spans - 3.0 * jnp.floor((spans + 0.5) * (1.0 / 3.0)))
        diagonal = lax.broadcasted_iota(jnp.int32, (seq, seq), 0) == lax.broadcasted_iota(jnp.int32, (seq, seq), 1)
        return jnp.sum(jnp.where(diagonal, phase, 0.0), axis=1, keepdims=True)

    def mix(l, h):
        arrived(sq_got.at[l, h], sq_recv.at[l, h])
        line = sq_sent[l, h]
        for o in range(1, n_dp):
            line = line + sq_got[l, h, o - 1]
        squares = jnp.sum(jnp.where(own_diag, line[:1, :], 0.0), axis=1, keepdims=True)
        inv_rms = lax.rsqrt(squares / (depth * n_dp) + NORM_EPS)

        def total(c):
            for g in range(len(GROUPS)):
                if GROUPS[g][0] == c:
                    arrived(got.at[l, h, :, :, columns_of(g)], rs_recv.at[l, h, g])
            cols = pl.ds(starts[c], sizes[c])
            out = sent[l, h, mine, cols].astype(F32)
            for o in range(1, n_dp):
                out = out + got[l, h, o - 1, :, cols].astype(F32)
            return out * inv_rms

        low_rank = total(0)
        z = offset[l : l + 1, :] + jnp.dot(
            jnp.tanh(low_rank[:, :rank]), decay_up[l], precision=lax.Precision.HIGHEST, preferred_element_type=F32
        )
        decay = to_rows(jnp.exp(sigmoid(z) * (-DECAY_SCALE) * pos[h * own : (h + 1) * own, :]), h, 0)
        learn = to_rows(
            sigmoid(
                jnp.dot(low_rank[:, rank:], rate_up[l], precision=lax.Precision.HIGHEST, preferred_element_type=F32)
            ),
            h,
            1,
        )
        keys = to_rows(total(1), h, 2)
        key_unit = keys * lax.rsqrt(half_sum(keys * keys) + 1.0)
        key_rate = key_unit * learn
        rows[h, 1] = key_rate
        query = to_rows(total(2), h, 3)
        key_query = half_sum(keys * query)
        rate_query = half_sum(key_rate * query)
        unit2 = twice(key_unit)
        query2 = twice(decay * query)
        if h == 0:
            loads[l, 5].wait()

        def products(t, acc):
            at = pl.ds(pl.multiple_of(t * TILE, TILE), TILE)
            s = state[l, h * count : (h + 1) * count, at]
            return (
                acc
                + jnp.dot((s * unit2).astype(BF16), gather1[at, :], preferred_element_type=F32)
                + jnp.dot((s * query2).astype(BF16), gather2[at, :], preferred_element_type=F32)
            )

        acc = lax.fori_loop(0, tiles, products, jnp.zeros((count, LANES), F32), unroll=True)
        turned = pltpu.roll(acc, HEAD, 1)
        state_key = jnp.where(low_rows, acc, turned)
        from_state = jnp.where(low_rows, turned, acc)
        value = to_rows(total(3), h, 4)
        readout = from_state - state_key * rate_query + value * key_query
        mean = half_sum(readout) * (1.0 / HEAD)
        centred = readout - mean
        var = half_sum(centred * centred) * (1.0 / HEAD)
        rows[h, 5] = centred * lax.rsqrt(var + GROUP_EPS)
        gate = sigmoid(total(4)) * head_gain[l : l + 1, :]
        normed = rows.at[h, 5]
        for j in range(width // LANES):
            even = normed[pl.ds(2 * j, own, stride=heads), :]
            odd = normed[pl.ds(2 * j + 1, own, stride=heads), :]
            cols = slice(j * LANES, (j + 1) * LANES)
            mixed_all[l, h, mine, cols] = (jnp.where(low, even, odd) * gate[:, cols]).astype(BF16)
        for o in range(1, n_dp):
            copy_of(
                mixed_all.at[l, h, mine], mixed_all.at[l, h, mine], ag_send, ag_recv.at[l, h], {"dp": dp_peer(o)}
            ).start()

        def split(v):
            high = v.astype(BF16)
            rest = (v - high.astype(F32)).astype(BF16)
            return jnp.where(low_rows, high.astype(F32), rest.astype(F32)).astype(BF16)

        splits[h, 0] = split(value)
        splits[h, 1] = split(state_key)

    def update(l, h, first, last):
        def one(t, carry):
            at = pl.ds(pl.multiple_of(t * TILE, TILE), TILE)
            wide = jnp.dot(splits[h, 0], spread[:, at], preferred_element_type=F32)
            drop = jnp.dot(splits[h, 1], spread[:, at], preferred_element_type=F32)
            block = slice(h * count, (h + 1) * count)
            state[l, block, at] = (
                state[l, block, at] * twice(rows[h, 0]) - drop * twice(rows[h, 1]) + wide * twice(rows[h, 2])
            )
            return carry

        lax.fori_loop(first, last, one, 0, unroll=True)

    def far_first(i):
        begin = jnp.where(lane_me < n_tp // 2, reducers // 2, 0)
        odd = lax.rem(lane_me, 2)
        turn = odd * (1 - 2 * (i % 2))
        return lax.rem(begin + i + turn + reducers, reducers)

    def output(l, h):
        arrived(mixed_all.at[l, h, : (n_dp - 1) * own], ag_recv.at[l, h])
        if h == 0:
            loads[l, 6].wait()
        product = jnp.dot(mixed_all[l, h], wo[l], preferred_element_type=F32).astype(BF16)
        for k in range(reducers):
            i, j = k // strips, k % strips
            terms[l, h, k] = product[
                i * part_rows : (i + 1) * part_rows, j * part_cols : (j + 1) * part_cols
            ]
        for i in range(reducers):
            k = far_first(i)
            copy = copy_of(
                terms.at[l, h, k], terms_got.at[l, h, lane_me], tr_send, tr_recv.at[l, h], {"tp": first + k}
            )
            pl.when(lane_me != first + k)(copy.start)

    reducing = (lane_me >= first) & (lane_me < first + reducers)
    slot = jnp.clip(lane_me - first, 0, reducers - 1)

    def gather_terms(l, h):
        @pl.when(reducing)
        def _():
            acc = terms[l, h, slot].astype(F32)
            if l == 0:
                at_rows = pl.ds(pl.multiple_of(slot // strips * part_rows, part_rows), part_rows)
                at_cols = pl.ds(pl.multiple_of(slot % strips * part_cols, part_cols), part_cols)
                acc = acc + x_ref[h, at_rows, at_cols].astype(F32)
            else:
                acc = acc + fresh[l - 1, h, slot].astype(F32)
            arrived(terms_got.at[l, h, : n_tp - 1], tr_recv.at[l, h])
            for o in range(1, n_tp):
                acc = acc + terms_got[l, h, tp_peer(o)].astype(F32)
            fresh[l, h, slot] = acc.astype(BF16)
            for o in range(1, n_tp):
                copy_of(
                    fresh.at[l, h, slot], fresh.at[l, h, slot], ta_send, ta_recv.at[l, h], {"tp": tp_peer(o)}
                ).start()

    def renew(l, h):
        @pl.when(reducing)
        def _():
            arrived(fresh.at[l, h, : reducers - 1], ta_recv.at[l, h])

        if reducers < n_tp:

            @pl.when(jnp.logical_not(reducing))
            def _():
                arrived(fresh.at[l, h], ta_recv.at[l, h])

    def finish(h):
        for i in range(reducers // strips):
            strip = [fresh[BLOCK_COUNT - 1, h, i * strips + j] for j in range(strips)]
            value = jnp.concatenate(strip, axis=1)
            for d in range(n_dp):
                low_row, high_row = max(d * own, i * part_rows), min((d + 1) * own, (i + 1) * part_rows)
                if low_row < high_row:
                    to = d * (seq - own) + h * own
                    stream_out[to + low_row : to + high_row, :] = value[
                        low_row - i * part_rows : high_row - i * part_rows, :
                    ]

    every = range(halves)
    cut = [tiles * i // 2 for i in range(3)]
    project_all()
    lax.fori_loop(0, tiles, fill, 0)
    pos = prepare()
    for l in range(BLOCK_COUNT):
        if l > 0:
            for h in every:
                renew(l - 1, h)
                project(l, h)
        if l + 1 < BLOCK_COUNT:
            load_in(l + 1)
            load_rest(l + 1)
        for h in every:
            mix(l, h)
        for h in every:
            output(l, h)
            update(l, h, cut[0], cut[1])
        for h in every:
            gather_terms(l, h)
            update(l, h, cut[1], cut[2])
    for h in every:
        renew(BLOCK_COUNT - 1, h)
        finish(h)
    left(got, rs_send)
    left(sq_got, sq_send)
    left(mixed_all.at[:, :, : (n_dp - 1) * own], ag_send)

    @pl.when(reducing)
    def _():
        left(terms.at[:, :, : reducers - 1], tr_send)
        left(terms_got.at[:, :, : n_tp - 1], ta_send)

    if reducers < n_tp:

        @pl.when(jnp.logical_not(reducing))
        def _():
            left(terms, tr_send)


def flush(out, state, out_hbm, state_hbm, sem):
    copies = [pltpu.make_async_copy(out, out_hbm, sem.at[0])]
    for i in range(FLUSHES):
        rows = state.shape[1] // FLUSHES
        at = pl.ds(i * rows, rows)
        copies.append(pltpu.make_async_copy(state.at[:, at], state_hbm.at[:, at], sem.at[i + 1]))
    for copy in copies:
        copy.start()
    for copy in copies:
        copy.wait()


def solution(mesh):
    n_dp, n_tp = mesh.shape["dp"], mesh.shape["tp"]

    def body(
        stream,
        history,
        input_norm_gain,
        query_weight,
        key_weight,
        value_weight,
        gate_weight,
        adapter_down_weight,
        decay_up_weight,
        rate_up_weight,
        decay_offset,
        head_norm_gain,
        output_weight,
        recurrent_state,
    ):
        batch, depth = stream.shape
        width = query_weight.shape[2]
        blocks, seq, heads, vk = recurrent_state.shape
        count = seq * heads
        halves = PIECES if seq % (8 * PIECES) == 0 else 1
        span = batch // halves
        own = seq // halves
        lanes = (span + LANES - 1) // LANES * LANES
        reducers = n_tp // 2 if n_tp % 4 == 0 else n_tp
        strips = min(reducers, depth // LANES)
        part_rows, part_cols = span * strips // reducers, depth // strips
        columns = 4 * width + adapter_down_weight.shape[2]
        vmem = pl.BlockSpec(memory_space=pltpu.VMEM)
        hbm = pl.BlockSpec(memory_space=pl.ANY)
        dma = pltpu.SemaphoreType.DMA

        def like(w):
            return pltpu.VMEM(w.shape, w.dtype)

        out, new_state = pl.pallas_call(
            functools.partial(kernel, n_dp, n_tp, halves),
            out_shape=(
                pltpu.VMEM((batch, depth), BF16),
                pltpu.VMEM((blocks, count, vk), F32),
            ),
            in_specs=[hbm] * 14,
            out_specs=(vmem, vmem),
            scratch_shapes=[
                like(stream),
                pltpu.VMEM((1, seq), history.dtype),
                like(input_norm_gain),
                like(decay_up_weight),
                like(rate_up_weight),
                like(decay_offset),
                like(head_norm_gain),
                like(adapter_down_weight),
                like(key_weight),
                like(query_weight),
                like(value_weight),
                like(gate_weight),
                like(output_weight),
                pltpu.VMEM((blocks, halves, span, columns), BF16),
                pltpu.VMEM((blocks, halves, n_dp - 1, own, columns), BF16),
                pltpu.VMEM((blocks, halves, 8, lanes), F32),
                pltpu.VMEM((blocks, halves, n_dp - 1, 8, lanes), F32),
                pltpu.VMEM((blocks, halves, span, width), BF16),
                pltpu.VMEM((blocks, halves, reducers, part_rows, part_cols), BF16),
                pltpu.VMEM((blocks, halves, n_tp, part_rows, part_cols), BF16),
                pltpu.VMEM((blocks, halves, reducers, part_rows, part_cols), BF16),
                pltpu.VMEM((halves, span, depth), BF16),
                pltpu.VMEM((halves, 6, count // halves, LANES), F32),
                pltpu.VMEM((halves, 2, count // halves, LANES), BF16),
                pltpu.VMEM((vk, LANES), BF16),
                pltpu.VMEM((vk, LANES), BF16),
                pltpu.VMEM((LANES, vk), BF16),
                dma((7,)),
                dma((blocks, 7)),
                dma,
                dma((blocks, halves, len(GROUPS))),
                dma,
                dma((blocks, halves)),
                dma,
                dma((blocks, halves)),
                dma,
                dma((blocks, halves)),
                dma,
                dma((blocks, halves)),
            ],
            compiler_params=pltpu.CompilerParams(
                collective_id=0, has_side_effects=True, vmem_limit_bytes=54 * 1024 * 1024
            ),
        )(
            stream,
            history[None, :],
            input_norm_gain,
            adapter_down_weight,
            key_weight,
            query_weight,
            value_weight,
            gate_weight,
            decay_up_weight,
            rate_up_weight,
            decay_offset,
            head_norm_gain,
            output_weight,
            recurrent_state.reshape(blocks, count, vk),
        )
        out, new_state = pl.pallas_call(
            flush,
            out_shape=(
                jax.ShapeDtypeStruct((batch, depth), BF16),
                jax.ShapeDtypeStruct((blocks, count, vk), F32),
            ),
            in_specs=[hbm, hbm],
            out_specs=(hbm, hbm),
            scratch_shapes=[dma((FLUSHES + 1,))],
            compiler_params=pltpu.CompilerParams(vmem_limit_bytes=1024 * 1024),
        )(out, new_state)
        return out, new_state.reshape(blocks, seq, heads, vk)

    placed = (
        P(None, "dp"),
        P("dp"),
        P(None, "dp"),
        P(None, "dp", "tp"),
        P(None, "dp", "tp"),
        P(None, "dp", "tp"),
        P(None, "dp", "tp"),
        P(None, "dp", None),
        P(None, None, "tp"),
        P(None, None, "tp"),
        P(None, "tp"),
        P(None, "tp"),
        P(None, "tp", "dp"),
        P(None, "dp", "tp", None),
    )
    return jax.shard_map(
        body,
        mesh=mesh,
        in_specs=placed,
        out_specs=(P(None, "dp"), P(None, "dp", "tp", None)),
        check_vma=False,
    )
```

```python
import functools

import jax
import jax.numpy as jnp
from jax import lax
from jax.experimental import pallas as pl
from jax.experimental.pallas import tpu as pltpu
from jax.sharding import PartitionSpec as P

HEAD = 64
SPAN = 64
BLOCK_COUNT = 2
LANES = 128
NORM_EPS = 0.25
GROUP_EPS = 0.25
DECAY_SCALE = 0.6065306597126334
TILE = 256
FLUSHES = 8
PIECES = 2
GROUPS = ((0, 1), (2,), (3, 4))
MESH = pl.DeviceIdType.MESH
F32 = jnp.float32
BF16 = jnp.bfloat16


def sigmoid(z):
    e = jnp.exp(-jnp.abs(z))
    return jnp.where(z >= 0, 1.0, e) / (1.0 + e)


def kernel(
    n_dp,
    n_tp,
    halves,
    stream_hbm,
    history_hbm,
    in_gain_hbm,
    adapter_hbm,
    key_hbm,
    query_hbm,
    value_hbm,
    gate_hbm,
    decay_up_hbm,
    rate_up_hbm,
    offset_hbm,
    head_gain_hbm,
    out_hbm,
    state_hbm,
    stream_out,
    state,
    stream_ref,
    history_ref,
    in_gain,
    decay_up,
    rate_up,
    offset,
    head_gain,
    wa,
    wk,
    wq,
    wv,
    wg,
    wo,
    sent,
    got,
    sq_sent,
    sq_got,
    mixed_all,
    terms,
    terms_got,
    fresh,
    x_ref,
    rows,
    splits,
    gather1,
    gather2,
    spread,
    small_sem,
    load_sem,
    rs_send,
    rs_recv,
    sq_send,
    sq_recv,
    ag_send,
    ag_recv,
    tr_send,
    tr_recv,
    ta_send,
    ta_recv,
):
    me = lax.axis_index("dp")
    lane_me = lax.axis_index("tp")
    batch, depth = stream_ref.shape
    seq = batch // n_dp
    width = wk.shape[2]
    heads = width // HEAD
    span = batch // halves
    own = seq // halves
    count = own * heads
    rank = wa.shape[2] // 2
    vk = state.shape[2]
    tiles = vk // TILE
    lanes = sq_sent.shape[3]
    reducers, part_rows, part_cols = terms.shape[2:]
    first = (n_tp - reducers) // 2
    strips = depth // part_cols

    def dp_peer(o):
        return lax.rem(me + o, n_dp)

    def tp_peer(o):
        return lax.rem(lane_me + o, n_tp)

    barrier = pltpu.get_barrier_semaphore()
    for o in range(1, n_tp):
        pl.semaphore_signal(barrier, inc=1, device_id={"tp": tp_peer(o)}, device_id_type=MESH)
    for o in range(1, n_dp):
        pl.semaphore_signal(barrier, inc=1, device_id={"dp": dp_peer(o)}, device_id_type=MESH)

    loads = {}
    small = []

    def load(l, i, src, dst):
        loads[l, i] = pltpu.make_async_copy(src.at[l], dst.at[l], load_sem.at[l, i])
        loads[l, i].start()

    def load_small(src, dst):
        small.append(pltpu.make_async_copy(src, dst, small_sem.at[len(small)]))
        small[-1].start()

    def load_in(l):
        load(l, 0, adapter_hbm, wa)
        load(l, 1, key_hbm, wk)
        load(l, 2, query_hbm, wq)
        load(l, 3, value_hbm, wv)
        load(l, 4, gate_hbm, wg)

    def load_rest(l):
        load(l, 5, state_hbm, state)
        load(l, 6, out_hbm, wo)

    load_small(stream_hbm, stream_ref)
    load_small(in_gain_hbm, in_gain)
    load_in(0)
    load_small(history_hbm, history_ref)
    load_small(decay_up_hbm, decay_up)
    load_small(rate_up_hbm, rate_up)
    load_small(offset_hbm, offset)
    load_small(head_gain_hbm, head_gain)
    load_rest(0)

    def fill(t, carry):
        at = pl.ds(pl.multiple_of(t * TILE, TILE), TILE)
        r = (lax.broadcasted_iota(jnp.int32, (TILE, LANES), 0) + t * TILE) // HEAD
        c = lax.broadcasted_iota(jnp.int32, (TILE, LANES), 1)
        gather1[at, :] = jnp.where(r == c, 1.0, 0.0).astype(BF16)
        gather2[at, :] = jnp.where(r + HEAD == c, 1.0, 0.0).astype(BF16)
        r = lax.broadcasted_iota(jnp.int32, (LANES, TILE), 0)
        c = (lax.broadcasted_iota(jnp.int32, (LANES, TILE), 1) + t * TILE) // HEAD
        spread[:, at] = jnp.where((r == c) | (r == c + HEAD), 1.0, 0.0).astype(BF16)
        return carry

    low = lax.broadcasted_iota(jnp.int32, (own, LANES), 1) < HEAD
    low_rows = lax.broadcasted_iota(jnp.int32, (count, LANES), 1) < HEAD

    def to_rows(value, h, i):
        buf = rows.at[h, i]
        for j in range(width // LANES):
            pair = value[:, j * LANES : (j + 1) * LANES]
            turned = pltpu.roll(pair, HEAD, 1)
            buf[pl.ds(2 * j, own, stride=heads), :] = jnp.where(low, pair, turned)
            buf[pl.ds(2 * j + 1, own, stride=heads), :] = jnp.where(low, turned, pair)
        return rows[h, i]

    def half_sum(v):
        return jnp.sum(v, axis=1, keepdims=True) * 0.5

    def twice(v):
        return jnp.concatenate([v, v], axis=1)

    mine = pl.ds(pl.multiple_of(me * own, own), own)
    row_at = lax.broadcasted_iota(jnp.int32, (span, lanes), 0)
    diag = row_at == lax.broadcasted_iota(jnp.int32, (span, lanes), 1)
    own_at = lax.broadcasted_iota(jnp.int32, (own, lanes), 0) + me * own
    own_diag = own_at == lax.broadcasted_iota(jnp.int32, (own, lanes), 1)
    sizes = [2 * rank, width, width, width, width]
    starts = [sum(sizes[:c]) for c in range(5)]
    def copy_of(src, dst, send, recv, where):
        return pltpu.make_async_remote_copy(
            src_ref=src, dst_ref=dst, send_sem=send, recv_sem=recv, device_id=where, device_id_type=MESH
        )

    def arrived(ref, recv):
        copy_of(ref, ref, tr_send, recv, {"tp": tp_peer(1)}).wait_recv()

    def left(ref, send):
        copy_of(ref, ref, send, ta_recv.at[0], {"tp": tp_peer(1)}).wait_send()

    def send_squares(l, h):
        for o in range(1, n_dp):
            copy_of(sq_sent.at[l, h], sq_got.at[l, h, o - 1], sq_send, sq_recv.at[h], {"dp": dp_peer(o)}).start()

    def columns_of(g):
        return pl.ds(starts[GROUPS[g][0]], sum(sizes[c] for c in GROUPS[g]))

    def send_columns(l, h, g):
        cols = columns_of(g)
        for o in range(1, n_dp):
            there = dp_peer(o)
            at = pl.ds(pl.multiple_of(there * own, own), own)
            copy_of(
                sent.at[l, h, at, cols], got.at[l, h, o - 1, :, cols], rs_send, rs_recv.at[h, g], {"dp": there}
            ).start()

    def put_squares(l, h, x):
        column = jnp.sum(x * x, axis=1, keepdims=True)
        line = jnp.sum(jnp.where(diag, column, 0.0), axis=0, keepdims=True)
        sq_sent[l, h] = jnp.broadcast_to(line, (8, lanes))

    weights = (wa, wk, wq, wv, wg)

    def project_all():
        small[0].wait()
        small[1].wait()
        for h in range(halves):
            for d in range(n_dp):
                x_ref[h, d * own : (d + 1) * own, :] = stream_ref[
                    d * seq + h * own : d * seq + (h + 1) * own, :
                ]
        for h in range(halves):
            put_squares(0, h, x_ref[h].astype(F32))
        x = x_ref[...].reshape(batch, depth).astype(F32)
        scaled = (x * in_gain[:1, :]).astype(BF16)
        for c, weight in enumerate(weights):
            loads[0, c].wait()
            cols = pl.ds(starts[c], sizes[c])
            product = jnp.dot(scaled, weight[0], preferred_element_type=F32).astype(BF16)
            sent[0, :, :, cols] = product.reshape(halves, span, sizes[c])
        pl.semaphore_wait(barrier, n_dp + n_tp - 2)
        for h in range(halves):
            send_squares(0, h)
            for g in range(len(GROUPS)):
                send_columns(0, h, g)

    def project(l, h):
        rows_of = []
        for i in range(reducers // strips):
            strip = [fresh[l - 1, h, i * strips + j] for j in range(strips)]
            rows_of.append(jnp.concatenate(strip, axis=1))
        x = jnp.concatenate(rows_of, axis=0).astype(F32)
        put_squares(l, h, x)
        scaled = (x * in_gain[l : l + 1, :]).astype(BF16)
        send_squares(l, h)
        for c, weight in enumerate(weights):
            if h == 0:
                loads[l, c].wait()
            cols = pl.ds(starts[c], sizes[c])
            sent[l, h, :, cols] = jnp.dot(scaled, weight[l], preferred_element_type=F32).astype(BF16)
            for g in range(len(GROUPS)):
                if GROUPS[g][-1] == c:
                    send_columns(l, h, g)

    def prepare():
        for copy in small[2:]:
            copy.wait()
        spans = jnp.floor(history_ref[...].astype(F32) * (1.0 / SPAN))
        phase = 0.5 + (spans - 3.0 * jnp.floor((spans + 0.5) * (1.0 / 3.0)))
        diagonal = lax.broadcasted_iota(jnp.int32, (seq, seq), 0) == lax.broadcasted_iota(jnp.int32, (seq, seq), 1)
        return jnp.sum(jnp.where(diagonal, phase, 0.0), axis=1, keepdims=True)

    def mix(l, h):
        arrived(sq_got.at[l, h], sq_recv.at[h])
        line = sq_sent[l, h]
        for o in range(1, n_dp):
            line = line + sq_got[l, h, o - 1]
        squares = jnp.sum(jnp.where(own_diag, line[:1, :], 0.0), axis=1, keepdims=True)
        inv_rms = lax.rsqrt(squares / (depth * n_dp) + NORM_EPS)

        def total(c):
            for g in range(len(GROUPS)):
                if GROUPS[g][0] == c:
                    arrived(got.at[l, h, :, :, columns_of(g)], rs_recv.at[h, g])
            cols = pl.ds(starts[c], sizes[c])
            out = sent[l, h, mine, cols].astype(F32)
            for o in range(1, n_dp):
                out = out + got[l, h, o - 1, :, cols].astype(F32)
            return out * inv_rms

        low_rank = total(0)
        z = offset[l : l + 1, :] + jnp.dot(
            jnp.tanh(low_rank[:, :rank]), decay_up[l], precision=lax.Precision.HIGHEST, preferred_element_type=F32
        )
        decay = to_rows(jnp.exp(sigmoid(z) * (-DECAY_SCALE) * pos[h * own : (h + 1) * own, :]), h, 0)
        learn = to_rows(
            sigmoid(
                jnp.dot(low_rank[:, rank:], rate_up[l], precision=lax.Precision.HIGHEST, preferred_element_type=F32)
            ),
            h,
            1,
        )
        keys = to_rows(total(1), h, 2)
        key_unit = keys * lax.rsqrt(half_sum(keys * keys) + 1.0)
        key_rate = key_unit * learn
        rows[h, 1] = key_rate
        query = to_rows(total(2), h, 3)
        key_query = half_sum(keys * query)
        rate_query = half_sum(key_rate * query)
        unit2 = twice(key_unit)
        query2 = twice(decay * query)
        if h == 0:
            loads[l, 5].wait()

        def products(t, acc):
            at = pl.ds(pl.multiple_of(t * TILE, TILE), TILE)
            s = state[l, h * count : (h + 1) * count, at]
            return (
                acc
                + jnp.dot((s * unit2).astype(BF16), gather1[at, :], preferred_element_type=F32)
                + jnp.dot((s * query2).astype(BF16), gather2[at, :], preferred_element_type=F32)
            )

        acc = lax.fori_loop(0, tiles, products, jnp.zeros((count, LANES), F32), unroll=True)
        turned = pltpu.roll(acc, HEAD, 1)
        state_key = jnp.where(low_rows, acc, turned)
        from_state = jnp.where(low_rows, turned, acc)
        value = to_rows(total(3), h, 4)
        readout = from_state - state_key * rate_query + value * key_query
        mean = half_sum(readout) * (1.0 / HEAD)
        centred = readout - mean
        var = half_sum(centred * centred) * (1.0 / HEAD)
        rows[h, 5] = centred * lax.rsqrt(var + GROUP_EPS)
        gate = sigmoid(total(4)) * head_gain[l : l + 1, :]
        normed = rows.at[h, 5]
        for j in range(width // LANES):
            even = normed[pl.ds(2 * j, own, stride=heads), :]
            odd = normed[pl.ds(2 * j + 1, own, stride=heads), :]
            cols = slice(j * LANES, (j + 1) * LANES)
            mixed_all[l, h, mine, cols] = (jnp.where(low, even, odd) * gate[:, cols]).astype(BF16)
        for o in range(1, n_dp):
            copy_of(
                mixed_all.at[l, h, mine], mixed_all.at[l, h, mine], ag_send, ag_recv.at[h], {"dp": dp_peer(o)}
            ).start()

        def split(v):
            high = v.astype(BF16)
            rest = (v - high.astype(F32)).astype(BF16)
            return jnp.where(low_rows, high.astype(F32), rest.astype(F32)).astype(BF16)

        splits[h, 0] = split(value)
        splits[h, 1] = split(state_key)

    def update(l, h, first, last):
        def one(t, carry):
            at = pl.ds(pl.multiple_of(t * TILE, TILE), TILE)
            wide = jnp.dot(splits[h, 0], spread[:, at], preferred_element_type=F32)
            drop = jnp.dot(splits[h, 1], spread[:, at], preferred_element_type=F32)
            block = slice(h * count, (h + 1) * count)
            state[l, block, at] = (
                state[l, block, at] * twice(rows[h, 0]) - drop * twice(rows[h, 1]) + wide * twice(rows[h, 2])
            )
            return carry

        lax.fori_loop(first, last, one, 0, unroll=True)

    def far_first(i):
        begin = jnp.where(lane_me < n_tp // 2, reducers // 2, 0)
        odd = lax.rem(lane_me, 2)
        turn = odd * (1 - 2 * (i % 2))
        return lax.rem(begin + i + turn + reducers, reducers)

    def output(l, h):
        arrived(mixed_all.at[l, h, : (n_dp - 1) * own], ag_recv.at[h])
        if h == 0:
            loads[l, 6].wait()
        product = jnp.dot(mixed_all[l, h], wo[l], preferred_element_type=F32).astype(BF16)
        for k in range(reducers):
            i, j = k // strips, k % strips
            terms[l, h, k] = product[
                i * part_rows : (i + 1) * part_rows, j * part_cols : (j + 1) * part_cols
            ]
        for i in range(reducers):
            k = far_first(i)
            copy = copy_of(
                terms.at[l, h, k], terms_got.at[l, h, lane_me], tr_send, tr_recv.at[h], {"tp": first + k}
            )
            pl.when(lane_me != first + k)(copy.start)

    reducing = (lane_me >= first) & (lane_me < first + reducers)
    slot = jnp.clip(lane_me - first, 0, reducers - 1)

    def gather_terms(l, h):
        @pl.when(reducing)
        def _():
            acc = terms[l, h, slot].astype(F32)
            if l == 0:
                at_rows = pl.ds(pl.multiple_of(slot // strips * part_rows, part_rows), part_rows)
                at_cols = pl.ds(pl.multiple_of(slot % strips * part_cols, part_cols), part_cols)
                acc = acc + x_ref[h, at_rows, at_cols].astype(F32)
            else:
                acc = acc + fresh[l - 1, h, slot].astype(F32)
            arrived(terms_got.at[l, h, : n_tp - 1], tr_recv.at[h])
            for o in range(1, n_tp):
                acc = acc + terms_got[l, h, tp_peer(o)].astype(F32)
            fresh[l, h, slot] = acc.astype(BF16)
            for o in range(1, n_tp):
                copy_of(
                    fresh.at[l, h, slot], fresh.at[l, h, slot], ta_send, ta_recv.at[h], {"tp": tp_peer(o)}
                ).start()

    def renew(l, h):
        @pl.when(reducing)
        def _():
            arrived(fresh.at[l, h, : reducers - 1], ta_recv.at[h])

        if reducers < n_tp:

            @pl.when(jnp.logical_not(reducing))
            def _():
                arrived(fresh.at[l, h], ta_recv.at[h])

    def finish(h):
        for i in range(reducers // strips):
            strip = [fresh[BLOCK_COUNT - 1, h, i * strips + j] for j in range(strips)]
            value = jnp.concatenate(strip, axis=1)
            for d in range(n_dp):
                low_row, high_row = max(d * own, i * part_rows), min((d + 1) * own, (i + 1) * part_rows)
                if low_row < high_row:
                    to = d * (seq - own) + h * own
                    stream_out[to + low_row : to + high_row, :] = value[
                        low_row - i * part_rows : high_row - i * part_rows, :
                    ]

    every = range(halves)
    cut = [tiles * i // 2 for i in range(3)]
    project_all()
    lax.fori_loop(0, tiles, fill, 0)
    pos = prepare()
    for l in range(BLOCK_COUNT):
        if l > 0:
            for h in every:
                renew(l - 1, h)
                project(l, h)
        if l + 1 < BLOCK_COUNT:
            load_in(l + 1)
            load_rest(l + 1)
        for h in every:
            mix(l, h)
        for h in every:
            output(l, h)
            update(l, h, cut[0], cut[1])
        for h in every:
            gather_terms(l, h)
            update(l, h, cut[1], cut[2])
    for h in every:
        renew(BLOCK_COUNT - 1, h)
        finish(h)
    left(got, rs_send)
    left(sq_got, sq_send)
    left(mixed_all.at[:, :, : (n_dp - 1) * own], ag_send)

    @pl.when(reducing)
    def _():
        left(terms.at[:, :, : reducers - 1], tr_send)
        left(terms_got.at[:, :, : n_tp - 1], ta_send)

    if reducers < n_tp:

        @pl.when(jnp.logical_not(reducing))
        def _():
            left(terms, tr_send)


def flush(out, state, out_hbm, state_hbm, sem):
    copies = [pltpu.make_async_copy(out, out_hbm, sem.at[0])]
    for i in range(FLUSHES):
        rows = state.shape[1] // FLUSHES
        at = pl.ds(i * rows, rows)
        copies.append(pltpu.make_async_copy(state.at[:, at], state_hbm.at[:, at], sem.at[i + 1]))
    for copy in copies:
        copy.start()
    for copy in copies:
        copy.wait()


def solution(mesh):
    n_dp, n_tp = mesh.shape["dp"], mesh.shape["tp"]

    def body(
        stream,
        history,
        input_norm_gain,
        query_weight,
        key_weight,
        value_weight,
        gate_weight,
        adapter_down_weight,
        decay_up_weight,
        rate_up_weight,
        decay_offset,
        head_norm_gain,
        output_weight,
        recurrent_state,
    ):
        batch, depth = stream.shape
        width = query_weight.shape[2]
        blocks, seq, heads, vk = recurrent_state.shape
        count = seq * heads
        halves = PIECES if seq % (8 * PIECES) == 0 else 1
        span = batch // halves
        own = seq // halves
        lanes = (span + LANES - 1) // LANES * LANES
        reducers = n_tp // 2 if n_tp % 4 == 0 else n_tp
        strips = min(reducers, depth // LANES)
        part_rows, part_cols = span * strips // reducers, depth // strips
        columns = 4 * width + adapter_down_weight.shape[2]
        vmem = pl.BlockSpec(memory_space=pltpu.VMEM)
        hbm = pl.BlockSpec(memory_space=pl.ANY)
        dma = pltpu.SemaphoreType.DMA

        def like(w):
            return pltpu.VMEM(w.shape, w.dtype)

        out, new_state = pl.pallas_call(
            functools.partial(kernel, n_dp, n_tp, halves),
            out_shape=(
                pltpu.VMEM((batch, depth), BF16),
                pltpu.VMEM((blocks, count, vk), F32),
            ),
            in_specs=[hbm] * 14,
            out_specs=(vmem, vmem),
            scratch_shapes=[
                like(stream),
                pltpu.VMEM((1, seq), history.dtype),
                like(input_norm_gain),
                like(decay_up_weight),
                like(rate_up_weight),
                like(decay_offset),
                like(head_norm_gain),
                like(adapter_down_weight),
                like(key_weight),
                like(query_weight),
                like(value_weight),
                like(gate_weight),
                like(output_weight),
                pltpu.VMEM((blocks, halves, span, columns), BF16),
                pltpu.VMEM((blocks, halves, n_dp - 1, own, columns), BF16),
                pltpu.VMEM((blocks, halves, 8, lanes), F32),
                pltpu.VMEM((blocks, halves, n_dp - 1, 8, lanes), F32),
                pltpu.VMEM((blocks, halves, span, width), BF16),
                pltpu.VMEM((blocks, halves, reducers, part_rows, part_cols), BF16),
                pltpu.VMEM((blocks, halves, n_tp, part_rows, part_cols), BF16),
                pltpu.VMEM((blocks, halves, reducers, part_rows, part_cols), BF16),
                pltpu.VMEM((halves, span, depth), BF16),
                pltpu.VMEM((halves, 6, count // halves, LANES), F32),
                pltpu.VMEM((halves, 2, count // halves, LANES), BF16),
                pltpu.VMEM((vk, LANES), BF16),
                pltpu.VMEM((vk, LANES), BF16),
                pltpu.VMEM((LANES, vk), BF16),
                dma((7,)),
                dma((blocks, 7)),
                dma,
                dma((halves, len(GROUPS))),
                dma,
                dma((halves,)),
                dma,
                dma((halves,)),
                dma,
                dma((halves,)),
                dma,
                dma((halves,)),
            ],
            compiler_params=pltpu.CompilerParams(
                collective_id=0, has_side_effects=True, vmem_limit_bytes=54 * 1024 * 1024
            ),
        )(
            stream,
            history[None, :],
            input_norm_gain,
            adapter_down_weight,
            key_weight,
            query_weight,
            value_weight,
            gate_weight,
            decay_up_weight,
            rate_up_weight,
            decay_offset,
            head_norm_gain,
            output_weight,
            recurrent_state.reshape(blocks, count, vk),
        )
        out, new_state = pl.pallas_call(
            flush,
            out_shape=(
                jax.ShapeDtypeStruct((batch, depth), BF16),
                jax.ShapeDtypeStruct((blocks, count, vk), F32),
            ),
            in_specs=[hbm, hbm],
            out_specs=(hbm, hbm),
            scratch_shapes=[dma((FLUSHES + 1,))],
            compiler_params=pltpu.CompilerParams(vmem_limit_bytes=1024 * 1024),
        )(out, new_state)
        return out, new_state.reshape(blocks, seq, heads, vk)

    placed = (
        P(None, "dp"),
        P("dp"),
        P(None, "dp"),
        P(None, "dp", "tp"),
        P(None, "dp", "tp"),
        P(None, "dp", "tp"),
        P(None, "dp", "tp"),
        P(None, "dp", None),
        P(None, None, "tp"),
        P(None, None, "tp"),
        P(None, "tp"),
        P(None, "tp"),
        P(None, "tp", "dp"),
        P(None, "dp", "tp", None),
    )
    return jax.shard_map(
        body,
        mesh=mesh,
        in_specs=placed,
        out_specs=(P(None, "dp"), P(None, "dp", "tp", None)),
        check_vma=False,
    )
```
